256 devices in a mesh: sp: 32 (over z, y), tp: 8 (over x, core).
Axes of the slice: x: 4, y: 4, z: 8, core: 2. Of those that a mesh axis runs over, the one named last changes fastest.
Arguments:
- latent: bfloat16 [12288, 2048], P(('sp', 'tp')), may hold values from -6 to 6
- context: bfloat16 [512, 2048], P('sp'), may hold values from -6 to 6
- cond_latent: float32 [2048], replicated, may hold values from -6 to 6
- cond_context: float32 [2048], replicated, may hold values from -12 to 12
- shift_weight: bfloat16 [2048, 2048], P('sp', 'tp'), may hold values from -0.125 to 0.125
- scale_weight: bfloat16 [2048, 2048], P('sp', 'tp'), may hold values from -0.125 to 0.125
- gate_weight: bfloat16 [2048, 2048], P('sp', 'tp'), may hold values from -0.125 to 0.125
- query_weight: bfloat16 [2, 2048, 1024], P(None, None, 'tp'), may hold values from -1.3258252 to 1.3258252
- key_weight: bfloat16 [2, 2048, 1024], P(None, None, 'tp'), may hold values from -1.3258252 to 1.3258252
- value_weight: bfloat16 [2048, 2048], P(None, 'tp'), may hold values from -0.125 to 0.125
- out_weight: bfloat16 [2048, 2048], P('tp'), may hold values from -0.125 to 0.125
- lambda_heads: float32 [16], P('tp'), may hold values from 0.3 to 0.8
- out_gain: float32 [2048], P('tp'), may hold values from 0.1 to 1.9
Outputs:
- result: bfloat16 [12288, 2048], P(('sp', 'tp'))
The draws below stay inside these ranges and needn't reach their ends.
All inputs are finite; a program needn't handle non-finite values.
Results may differ from the reference program's by a relative error of at most 0.02.
The reference program's roundings to bfloat16 on the way count: a program that leaves them out, or rounds other values in their place, can miss the bound.
Values may be sent and summed in bfloat16 or wider, within the bound.
A program may use at most 128 MiB of HBM per device.

```python
import math
import jax
import jax.numpy as jnp
from jax import lax

D = 2048
HEADS = 16
HEAD_DIM = 64
GRID_W = 64
CTX = 512
VALUE_DIM = 128
TOKENS = 12288
N_TP = 8


def projection(key, salt_value):
    entries = jax.random.truncated_normal(jax.random.fold_in(key, salt_value), -6.0, 6.0, (2, D, HEADS, HEAD_DIM), jnp.float32)
    scaled = entries * D ** (-0.5)
    return scaled.reshape(2, D, HEADS * HEAD_DIM).astype(jnp.bfloat16)


def draw_query_weight(key, part):
    return projection(key, 11)


def draw_key_weight(key, part):
    return projection(key, 23)


def level_of(own_key, extent, shards, low, top_value):
    gain = 1.0
    for dim, shards_of in shards:
        steps = jax.random.uniform(jax.random.fold_in(jax.random.fold_in(own_key, 6), dim), (shards_of,), jnp.float32, low / len(shards), top_value / len(shards))
        gain = gain * jnp.repeat(jnp.exp(steps), extent[dim] // shards_of).reshape((-1,) + (1,) * (len(extent) - 1 - dim))
    return gain


def gaussian(stream_key, extent, spread, reach, cuts=(), held_as=jnp.bfloat16):
    values = spread * jax.random.normal(stream_key, extent, jnp.float32)
    if cuts:
        values = values * level_of(stream_key, extent, cuts, -0.22, 0.18)
    return jnp.clip(values, -reach, reach).astype(held_as)


def setup_inputs(seed: int = 0) -> dict:
    streams_of = jax.random.split(jax.random.key(seed), 14)
    latent = gaussian(streams_of[0], (TOKENS, D), 1.0, 6.0, ((0, 256),))
    context = gaussian(streams_of[1], (CTX, D), 1.0, 6.0, ((0, 32),))
    cond_latent = gaussian(streams_of[2], (D,), 1.0, 6.0, (), jnp.float32)
    cond_context = gaussian(streams_of[3], (D,), 2.0, 12.0, (), jnp.float32)
    shift_weight = gaussian(streams_of[4], (D, D), D ** -0.5, 0.125, ((0, 32), (1, 8)))
    scale_weight = gaussian(streams_of[5], (D, D), D ** -0.5, 0.125, ((0, 32), (1, 8)))
    gate_weight = gaussian(streams_of[6], (D, D), D ** -0.5, 0.125, ((0, 32), (1, 8)))
    query_weight = draw_query_weight(jax.random.fold_in(streams_of[13], 71), 0)
    key_weight = draw_key_weight(jax.random.fold_in(streams_of[13], 71), 0)
    value_weight = gaussian(streams_of[9], (D, HEADS * VALUE_DIM), D ** -0.5, 0.125, ((1, 8),))
    out_weight = gaussian(streams_of[10], (HEADS * VALUE_DIM, D), (HEADS * VALUE_DIM) ** -0.5, 0.125, ((0, 8),))
    lambda_heads = jnp.clip(0.3 + 0.5 * jax.random.uniform(streams_of[11], (HEADS,), jnp.float32) ** level_of(streams_of[11], (HEADS,), ((0, 8),), -0.2, 0.2), 0.3, 0.8)
    out_gain = jnp.clip(1.0 + 0.18 * jax.random.normal(streams_of[12], (HEADS * VALUE_DIM,), jnp.float32), 0.1, 1.9)
    return dict(latent=latent, context=context, cond_latent=cond_latent, cond_context=cond_context, shift_weight=shift_weight, scale_weight=scale_weight, gate_weight=gate_weight, query_weight=query_weight, key_weight=key_weight, value_weight=value_weight, out_weight=out_weight, lambda_heads=lambda_heads, out_gain=out_gain)


norm_eps = 1e-06
rope_theta = 10000.0

def rms_scale(matrix):
    return matrix * lax.rsqrt(lax.optimization_barrier(jnp.mean(matrix * matrix, axis=-1, keepdims=True)) + norm_eps)

def modulated(activations, shift, scale):
    return (rms_scale(activations.astype(jnp.float32)) * (1.0 + scale) + shift).astype(jnp.bfloat16)

def rotate(vectors, positions, grid_width):
    quarter = vectors.shape[-1] // 4
    inverse = rope_theta ** (-jnp.arange(quarter, dtype=jnp.float32) / quarter)
    grid_row = (positions // grid_width).astype(jnp.float32)
    grid_col = (positions % grid_width).astype(jnp.float32)
    angles = jnp.concatenate([grid_row[:, None] * inverse, grid_col[:, None] * inverse], axis=-1)
    cos_table = jnp.cos(angles)[:, None, :]
    sin_table = jnp.sin(angles)[:, None, :]
    former = vectors[..., :2 * quarter]
    latter = vectors[..., 2 * quarter:]
    return jnp.concatenate([former * cos_table - latter * sin_table, latter * cos_table + former * sin_table], axis=-1)

def reference(latent, context, cond_latent, cond_context, shift_weight, scale_weight, gate_weight, query_weight, key_weight, value_weight, out_weight, lambda_heads, out_gain):
    conditions = jax.nn.silu(jnp.stack([cond_latent, cond_context])).astype(jnp.bfloat16)
    shifts = jnp.dot(conditions, shift_weight, preferred_element_type=jnp.float32)
    scales = jnp.dot(conditions, scale_weight, preferred_element_type=jnp.float32)
    gate_vector = jnp.dot(conditions[:1], gate_weight, preferred_element_type=jnp.float32)[0]
    hidden = modulated(latent, shifts[0], scales[0])
    context_hidden = modulated(context, shifts[1], scales[1])
    positions = jnp.arange(TOKENS, dtype=jnp.int32)

    def latent_heads(weight):
        product = jnp.dot(hidden, weight, preferred_element_type=jnp.float32).reshape(TOKENS, HEADS, HEAD_DIM)
        return rotate(product, positions, GRID_W).astype(jnp.bfloat16)

    def context_heads(weight):
        product = jnp.dot(context_hidden, weight, preferred_element_type=jnp.float32)
        return product.reshape(CTX, HEADS, HEAD_DIM).astype(jnp.bfloat16)
    queries = jnp.stack([latent_heads(query_weight[0]), latent_heads(query_weight[1])])
    key_rows = jnp.stack([jnp.concatenate([context_heads(key_weight[which_map]), latent_heads(key_weight[which_map])], axis=0) for which_map in (0, 1)])
    value_rows = jnp.concatenate([jnp.dot(context_hidden, value_weight, preferred_element_type=jnp.float32).astype(jnp.bfloat16), jnp.dot(hidden, value_weight, preferred_element_type=jnp.float32).astype(jnp.bfloat16)], axis=0)
    queries, key_rows, value_rows = lax.optimization_barrier((queries, key_rows, value_rows))
    queries = queries.transpose(2, 0, 1, 3)
    key_rows = key_rows.transpose(2, 0, 1, 3)
    value_rows = value_rows.reshape(CTX + TOKENS, HEADS, VALUE_DIM).transpose(1, 0, 2)
    query_block = math.gcd(TOKENS, 512)

    def one_head(operands):
        head_queries, head_keys, head_values, head_lambda = operands
        key_float = head_keys.astype(jnp.float32)
        value_float = head_values.astype(jnp.float32)
        blocks = head_queries.reshape(2, TOKENS // query_block, query_block, HEAD_DIM).transpose(1, 0, 2, 3)

        def one_block(block_queries):
            scores = jnp.einsum('mqd,mkd->mqk', block_queries.astype(jnp.float32), key_float) * HEAD_DIM ** (-0.5)
            weights = jnp.exp(scores - lax.optimization_barrier(jnp.max(scores, axis=-1, keepdims=True)))
            totals = lax.optimization_barrier(jnp.sum(weights, axis=-1, keepdims=True))
            rounded = lax.optimization_barrier(weights.astype(jnp.bfloat16)).astype(jnp.float32)
            numerator = jnp.einsum('mqk,ke->mqe', rounded, value_float)
            return numerator[0] / totals[0] - head_lambda * (numerator[1] / totals[1])
        return lax.map(one_block, blocks).reshape(TOKENS, VALUE_DIM)
    mixed = lax.map(one_head, (queries, key_rows, value_rows, lambda_heads))
    normed = rms_scale(mixed) * out_gain.reshape(HEADS, 1, VALUE_DIM)
    heads_out = normed.transpose(1, 0, 2).reshape(TOKENS, HEADS * VALUE_DIM).astype(jnp.bfloat16)
    group_width = HEADS // N_TP * VALUE_DIM
    summed = jnp.zeros((TOKENS, D), jnp.float32)
    for group_index in range(N_TP):
        lower = group_index * group_width
        group_term = jnp.dot(heads_out[:, lower:lower + group_width], out_weight[lower:lower + group_width], preferred_element_type=jnp.float32)
        summed = summed + lax.optimization_barrier(group_term.astype(jnp.bfloat16)).astype(jnp.float32)
    return (latent.astype(jnp.float32) + gate_vector * summed).astype(jnp.bfloat16)
```

```python
import functools

import jax
import jax.numpy as jnp
from jax import lax
from jax.experimental import pallas as pl
from jax.experimental.pallas import tpu as pltpu
from jax.sharding import PartitionSpec as P

HEAD_DIM = 64
GRID_W = 64
VALUE_DIM = 128
NX, NY, NZ, NC = 4, 4, 8, 2

norm_eps = 1e-06
rope_theta = 10000.0
log2_e = 1.4426950408889634

MESH = pl.DeviceIdType.MESH
F32, BF16 = jnp.float32, jnp.bfloat16
NT = (((1,), (1,)), ((), ()))


def send(src, dst, send_sem, recv_sem, device):
    pltpu.make_async_remote_copy(
        src_ref=src, dst_ref=dst, send_sem=send_sem, recv_sem=recv_sem,
        device_id=device, device_id_type=MESH,
    ).start()


def landed(ref, sem):
    pltpu.make_async_copy(ref, ref, sem).wait()


class Around:
    def __init__(self, buf, first, second, sems, x, c, place):
        self.buf, self.first, self.second, self.place = buf, first, second, place
        self.send, self.recv, self.dsend, self.drecv = sems
        self.c = c
        self.x = x
        self.xl, self.xr, self.xa = (x + 3) % NX, (x + 1) % NX, (x + 2) % NX

    def at(self, x, c=None):
        return self.buf.at[x * NC + (self.c if c is None else c)]

    def start(self, src):
        own, other = self.at(self.x), self.place(self.x, 1 - self.c)
        send(src, own, self.send.at[0], self.recv.at[0], self.place(self.xr, self.c))
        send(src, own, self.send.at[1], self.recv.at[1], self.place(self.xl, self.c))
        send(src, own, self.dsend.at[0], self.drecv.at[0], other)

    def forward(self):
        left, right, other = self.at(self.xl), self.at(self.xr), self.place(self.x, 1 - self.c)
        landed(left, self.recv.at[0])
        a = self.first(left)
        send(a, a, self.send.at[2], self.recv.at[2], self.place(self.xr, self.c))
        landed(right, self.recv.at[1])
        b = self.second(right)
        send(b, b, self.send.at[3], self.recv.at[3], self.place(self.xl, self.c))
        send(left, left, self.dsend.at[1], self.drecv.at[1], other)
        send(right, right, self.dsend.at[2], self.drecv.at[2], other)

    def last(self):
        far, other = self.at(self.xa), self.place(self.x, 1 - self.c)
        landed(self.first(far), self.recv.at[2])
        landed(self.second(far), self.recv.at[3])
        send(far, far, self.dsend.at[3], self.drecv.at[3], other)

    def finish(self):
        for k, at in enumerate((self.x, self.xl, self.xr, self.xa)):
            landed(self.at(at, 1 - self.c), self.drecv.at[k])

    def drain(self, src):
        landed(src, self.send.at[0])
        landed(src, self.send.at[1])
        landed(src, self.dsend.at[0])
        landed(self.first(self.at(self.xl)), self.send.at[2])
        landed(self.second(self.at(self.xr)), self.send.at[3])
        for k, at in enumerate((self.xl, self.xr, self.xa)):
            landed(self.at(at), self.dsend.at[k + 1])


def attend(qs, m, acc, k, v, sbuf, block):
    n = qs.shape[0] // block
    width = k.shape[0]
    v1 = jnp.concatenate([v, jnp.ones(v.shape, v.dtype)], axis=1)

    def scores(i):
        return lax.dot_general(qs[pl.ds(i * block, block), :], k, NT, preferred_element_type=F32)

    sbuf[0, :, :width] = scores(0)
    for i in range(n):
        if i + 1 < n:
            sbuf[(i + 1) % 2, :, :width] = scores(i + 1)
        rows = pl.ds(i * block, block)
        s = sbuf[i % 2, :, :width]
        before = m[rows, :]
        after = jnp.maximum(before, jnp.max(s, axis=1, keepdims=True))
        p = jnp.exp2(s - after[:, :1]).astype(BF16)
        rescale = jnp.exp2(before - after)
        m[rows, :] = after
        pv = jnp.dot(p, v1, preferred_element_type=F32)
        acc[rows, :] = acc[rows, :] * jnp.concatenate([rescale, rescale], axis=1) + pv


def kernel(
    tok, ctxr,
    lat, ctx, lhs, shw, scw, gaw, extra, cos, sin, wq, wk, wv, wo, out,
    zbuf, ybuf, tbuf, modw, lbuf, hid, w, wall, qst, kst, vst, qbuf, kv, qs, m, acc, sbuf, obuf, hb,
    wsem, zs_s, zs_r, ys_s, ys_r, ts_s, ts_r,
    l_s, l_r, l_ds, l_dr, w_s, w_r, w_ds, w_dr,
    q_s, q_r, k_s, v_s, kv_r, own_s, fwd_s, ring_r, d_s, d_r, o_s, o_r,
):
    sp, tp = lax.axis_index("sp"), lax.axis_index("tp")
    z, y = sp // NY, sp % NY
    x, c = tp // NC, tp % NC

    def place(px, pc, py=None, pz=None):
        return ((z if pz is None else pz) * NY + (y if py is None else py), px * NC + pc)

    loads = [
        pltpu.make_async_copy(wo, wall.at[tp], wsem.at[0]),
        pltpu.make_async_copy(wq.at[0], w.at[:, pl.ds(0, 128)], wsem.at[1]),
        pltpu.make_async_copy(wq.at[1], w.at[:, pl.ds(128, 128)], wsem.at[2]),
        pltpu.make_async_copy(wk.at[0], w.at[:, pl.ds(256, 128)], wsem.at[3]),
        pltpu.make_async_copy(wk.at[1], w.at[:, pl.ds(384, 128)], wsem.at[4]),
        pltpu.make_async_copy(wv, w.at[:, pl.ds(512, 256)], wsem.at[5]),
    ]
    for load in loads:
        load.start()

    barrier = pltpu.get_barrier_semaphore()
    others = [(dx, dy, dc) for dx in range(NX) for dy in range(NY) for dc in range(NC)][1:]
    for dz in range(1, NZ):
        pl.semaphore_signal(barrier, inc=1, device_id=place(x, c, pz=(z + dz) % NZ), device_id_type=MESH)
    for dx, dy, dc in others:
        pl.semaphore_signal(
            barrier, inc=1, device_id=place((x + dx) % NX, (c + dc) % NC, py=(y + dy) % NY), device_id_type=MESH
        )

    part = jnp.dot(lhs[0], shw[...], preferred_element_type=F32)
    part += jnp.dot(lhs[1], scw[...], preferred_element_type=F32)
    part += jnp.dot(lhs[2], gaw[...], preferred_element_type=F32)
    zbuf[z] = part[:8]
    lbuf[tp] = lat[...]

    pl.semaphore_wait(barrier, NZ - 1 + len(others))

    for d in range(1, NZ):
        send(zbuf.at[z], zbuf.at[z], zs_s.at[d - 1], zs_r.at[d - 1], place(x, c, pz=(z + d) % NZ))
    rows = Around(
        lbuf, lambda r: r.at[:, pl.ds(0, 1024)], lambda r: r.at[:, pl.ds(1024, 1024)], (l_s, l_r, l_ds, l_dr), x, c, place
    )
    rows.start(lat)
    for d in range(1, NZ):
        landed(zbuf.at[(z - d + NZ) % NZ], zs_r.at[d - 1])
    total = zbuf[0]
    for k in range(1, NZ):
        total += zbuf[k]
    ybuf[y] = total
    for d in range(1, NY):
        send(ybuf.at[y], ybuf.at[y], ys_s.at[d - 1], ys_r.at[d - 1], place(x, c, py=(y + d) % NY))
    for d in range(1, NY):
        landed(ybuf.at[(y - d + NY) % NY], ys_r.at[d - 1])
    tbuf[tp] = (ybuf[0] + ybuf[1]) + (ybuf[2] + ybuf[3]) + extra[...]
    tps = [(dx, dc) for dx in range(NX) for dc in range(NC)][1:]
    for k, (dx, dc) in enumerate(tps):
        send(tbuf.at[tp], tbuf.at[tp], ts_s.at[k], ts_r.at[k], place((x + dx) % NX, (c + dc) % NC))
    rows.forward()
    for k, (dx, dc) in enumerate(tps):
        landed(tbuf.at[((x - dx + NX) % NX) * NC + (c + dc) % NC], ts_r.at[k])
    for k in range(NX * NC):
        modw[:, k * 256 : (k + 1) * 256] = tbuf[k]
    rows.last()

    loads[0].wait()
    weights = Around(
        wall, lambda r: r.at[pl.ds(0, 128)], lambda r: r.at[pl.ds(128, 128)], (w_s, w_r, w_ds, w_dr), x, c, place
    )
    weights.start(wall.at[tp])
    rows.finish()

    def modulate(values, shift, scale):
        values = values.astype(F32)
        inverse = lax.rsqrt(jnp.mean(values * values, axis=-1, keepdims=True) + norm_eps)
        return (values * inverse * (1.0 + scale) + shift).astype(BF16)

    own_rows = lat.shape[0]

    def one_block(k, _):
        hid[pl.ds(pl.multiple_of(k * own_rows, 16), own_rows), :] = modulate(lbuf[k], modw[0:1, :], modw[2:3, :])
        return 0

    lax.fori_loop(0, NX * NC, one_block, 0)
    hid[tok : tok + ctxr, :] = modulate(ctx[...], modw[1:2, :], modw[3:4, :])
    for load in loads[1:]:
        load.wait()

    lane = lax.broadcasted_iota(jnp.int32, (tok + ctxr, 128), 1)
    low_half, low_head = lane % 64 < 32, lane < 64

    def turned(u):
        swapped = jnp.where(low_half, pltpu.roll(u, 96, 1), pltpu.roll(u, 32, 1))
        return u * cos[...] + swapped * sin[...]

    def by_head(both):
        m1, m2 = turned(both[:, :128]), turned(both[:, 128:])
        return (
            jnp.where(low_head, m1, pltpu.roll(m2, 64, 1)),
            jnp.where(low_head, pltpu.roll(m1, 64, 1), m2),
        )

    keys = by_head(jnp.dot(hid[...], w[:, 256:512], preferred_element_type=F32))
    kst[0], kst[1] = keys[0].astype(BF16), keys[1].astype(BF16)
    vals = jnp.dot(hid[...], w[:, 512:768], preferred_element_type=F32).astype(BF16)
    vst[0], vst[1] = vals[:, :128], vals[:, 128:]

    def self_head(j):
        return 2 * c + j == y

    for j in range(2):
        yd = 2 * c + j
        off = (y - yd + NY) % NY

        @pl.when(jnp.logical_or(yd != y, c != 0))
        def _():
            send(kst.at[j], kv.at[0, z, off], k_s.at[j], kv_r.at[off], place(x, 0, py=yd))

        @pl.when(jnp.logical_and(yd == y, c == 0))
        def _():
            kv[0, z, 0] = kst[j]

        @pl.when(jnp.logical_or(yd != y, c != 1))
        def _():
            send(vst.at[j], kv.at[1, z, off], v_s.at[j], kv_r.at[off], place(x, 1, py=yd))

        @pl.when(jnp.logical_and(yd == y, c == 1))
        def _():
            kv[1, z, 0] = vst[j]

    heads = by_head(jnp.dot(hid[...], w[:, 0:256], preferred_element_type=F32))
    for j in range(2):
        qst[j] = (heads[j][:tok] * (log2_e * HEAD_DIM**-0.5)).astype(BF16)
    for j in range(2):
        yd = 2 * c + j

        @pl.when(yd != y)
        def _():
            send(qst.at[j], qbuf.at[y % 2], q_s.at[j], q_r.at[y % 2], place(x, y // 2, py=yd))

        @pl.when(yd == y)
        def _():
            qbuf[y % 2] = qst[j]

    m[...] = jnp.full(m.shape, -jnp.inf, F32)
    acc[...] = jnp.zeros(acc.shape, F32)

    up, down, other = place(x, c, pz=(z + 1) % NZ), place(x, c, pz=(z + NZ - 1) % NZ), place(x, 1 - c)

    def half(zs, p):
        return kv.at[c, zs, pl.ds(2 * p, 2)]

    for p in range(2):
        if p == 0:

            @pl.when(c != y // 2)
            def _():
                landed(kv.at[c, z, 0], kv_r.at[0])
        else:
            landed(kv.at[c, z, 2], kv_r.at[2])
        landed(kv.at[c, z, 2 * p + 1], kv_r.at[2 * p + 1])
        mine = half(z, p)
        send(mine, mine, own_s.at[0, p], ring_r.at[1, p], up)
        send(mine, mine, own_s.at[1, p], ring_r.at[2, p], down)
        send(mine, mine, d_s.at[0, p], d_r.at[0, p], other)

    for i in range(2):

        @pl.when(2 * c + i != y)
        def _():
            landed(qbuf.at[i], q_r.at[i])

    low = lax.broadcasted_iota(jnp.int32, (tok, 128), 1) < 64
    for i in range(2):
        q = qbuf[i]
        nothing = jnp.zeros_like(q)
        qs[i * tok : (i + 1) * tok, :] = jnp.where(low, q, nothing)
        qs[(2 + i) * tok : (3 + i) * tok, :] = jnp.where(low, nothing, q)

    def source(u):
        return (z + (2 * ((u + 1) % 2) - 1) * ((u + 1) // 2) + NZ) % NZ

    def chunk(u, _):
        @pl.when(u == 4)
        def _():
            weights.forward()

        @pl.when(u == 6)
        def _():
            weights.last()

        zs = source(u)
        for p in range(2):
            piece = half(zs, p)

            @pl.when(u >= 1)
            def _():
                landed(piece, ring_r.at[u, p])
                if p == 0:
                    goes, later = u <= 5, u + 2
                else:
                    goes, later = jnp.logical_or(u <= 4, u == 6), u + 2 - u // 6
                side = (u + 1) % 2
                nz = (z + 1 - 2 * side + NZ) % NZ

                @pl.when(goes)
                def _():
                    send(piece, piece, fwd_s.at[u, p], ring_r.at[later, p], place(x, c, pz=nz))

                send(piece, piece, d_s.at[u, p], d_r.at[u, p], other)

        for p in range(2):
            landed(kv.at[1 - c, zs, pl.ds(2 * p, 2)], d_r.at[u, p])
        k = kv[0, zs, :, 0:tok, :].reshape(NY * tok, 128)
        v = kv[1, zs, :, 0:tok, :].reshape(NY * tok, 128)
        attend(qs, m, acc, k, v, sbuf, sbuf.shape[1])
        return 0

    lax.fori_loop(0, NZ, chunk, 0)
    k = kv[0, :, :, tok:, :].reshape(NZ * NY * ctxr, 128)
    v = kv[1, :, :, tok:, :].reshape(NZ * NY * ctxr, 128)
    attend(qs, m, acc, k, v, sbuf, sbuf.shape[1])

    both = 2 * tok
    mine = tbuf[2 * x + y // 2]
    picked = jnp.where(y % 2 == 0, mine[:, :128], mine[:, 128:])
    gain, factor = picked[5:6, :], picked[6:7, :]
    mixed = acc[:both, :128] / acc[:both, 128:] - factor * (acc[both:, :128] / acc[both:, 128:])
    normed = mixed * lax.rsqrt(jnp.mean(mixed * mixed, axis=-1, keepdims=True) + norm_eps) * gain
    obuf[...] = normed.astype(BF16).reshape(obuf.shape)
    head = 4 * x + y
    for i in range(2):
        for t in range(NX * NC):
            home = jnp.logical_and(2 * c + i == y, tp == t)

            @pl.when(jnp.logical_not(home))
            def _():
                send(
                    obuf.at[i, t], hb.at[head], o_s.at[i, t], o_r.at[head], (z * NY + 2 * c + i, t)
                )

            @pl.when(home)
            def _():
                hb[head] = obuf[i, t]

    weights.finish()
    for h in range(NX * NY):
        hx, hy = h // NY, h % NY

        @pl.when(jnp.logical_not(jnp.logical_and(jnp.logical_and(hx == x, hy == y), y // 2 == c)))
        def _():
            landed(hb.at[h], o_r.at[h])

    mixed_sum = jnp.zeros((own_rows, wall.shape[2]), F32)
    for g in range(NX * NC):
        pair = jnp.concatenate([hb[2 * g], hb[2 * g + 1]], axis=1)
        mixed_sum += jnp.dot(pair, wall[g], preferred_element_type=F32).astype(BF16).astype(F32)
    out[...] = (lat[...].astype(F32) + modw[4:5, :] * mixed_sum).astype(BF16)

    for d in range(1, NZ):
        landed(zbuf.at[z], zs_s.at[d - 1])
    for d in range(1, NY):
        landed(ybuf.at[y], ys_s.at[d - 1])
    for k in range(len(tps)):
        landed(tbuf.at[tp], ts_s.at[k])
    rows.drain(lat)
    weights.drain(wall.at[tp])
    for j in range(2):
        yd = 2 * c + j

        @pl.when(yd != y)
        def _():
            landed(qst.at[j], q_s.at[j])

        @pl.when(jnp.logical_or(yd != y, c != 0))
        def _():
            landed(kst.at[j], k_s.at[j])

        @pl.when(jnp.logical_or(yd != y, c != 1))
        def _():
            landed(vst.at[j], v_s.at[j])

    for p in range(2):
        for side in range(2):
            landed(half(z, p), own_s.at[side, p])
        for u in range(NZ):
            landed(half(z, p), d_s.at[u, p])
            if u >= 1 and (u <= 5 if p == 0 else u <= 4 or u == 6):
                landed(half(z, p), fwd_s.at[u, p])
    for i in range(2):
        for t in range(NX * NC):

            @pl.when(jnp.logical_not(jnp.logical_and(2 * c + i == y, tp == t)))
            def _():
                landed(obuf.at[i, t], o_s.at[i, t])


def tables(sp, tok, ctxr):
    quarter = HEAD_DIM // 4
    inverse = rope_theta ** (-jnp.arange(quarter, dtype=F32) / quarter)
    positions = sp * tok + jnp.arange(tok, dtype=jnp.int32)
    grid_row = (positions // GRID_W).astype(F32)
    grid_col = (positions % GRID_W).astype(F32)
    angles = jnp.concatenate([grid_row[:, None] * inverse, grid_col[:, None] * inverse], axis=-1)
    cos, sin = jnp.cos(angles), jnp.sin(angles)
    cos = jnp.concatenate([cos, cos, cos, cos], axis=-1)
    sin = jnp.concatenate([-sin, sin, -sin, sin], axis=-1)
    return (
        jnp.concatenate([cos, jnp.ones((ctxr, 128), F32)], axis=0),
        jnp.concatenate([sin, jnp.zeros((ctxr, 128), F32)], axis=0),
    )


def local(
    latent, context, cond_latent, cond_context, shift_weight, scale_weight, gate_weight,
    query_weight, key_weight, value_weight, out_weight, lambda_heads, out_gain,
):
    own_rows, width = latent.shape
    ctxr = context.shape[0]
    tok = own_rows * NX * NC
    sp = lax.axis_index("sp")
    mod_rows = shift_weight.shape[0]
    conditions = jnp.stack([cond_latent, cond_context])
    conditions = jax.nn.silu(lax.dynamic_slice_in_dim(conditions, sp * mod_rows, mod_rows, 1)).astype(BF16)
    lhs = jnp.stack(
        [
            jnp.pad(conditions, ((0, 14), (0, 0))),
            jnp.pad(conditions, ((2, 12), (0, 0))),
            jnp.pad(conditions[:1], ((4, 11), (0, 0))),
        ]
    )
    extra = jnp.concatenate(
        [
            jnp.zeros((5, 256), F32),
            out_gain[None],
            jnp.repeat(lambda_heads, VALUE_DIM)[None],
            jnp.zeros((1, 256), F32),
        ],
        axis=0,
    )
    cos, sin = tables(sp, tok, ctxr)
    vmem = pl.BlockSpec(memory_space=pltpu.VMEM)
    hbm = pl.BlockSpec(memory_space=pl.ANY)
    dma = pltpu.SemaphoreType.DMA
    block = 256
    return pl.pallas_call(
        functools.partial(kernel, tok, ctxr),
        out_shape=jax.ShapeDtypeStruct((own_rows, width), BF16),
        in_specs=[vmem] * 9 + [hbm] * 4,
        out_specs=vmem,
        scratch_shapes=[
            pltpu.VMEM((NZ, 8, 256), F32),
            pltpu.VMEM((NY, 8, 256), F32),
            pltpu.VMEM((NX * NC, 8, 256), F32),
            pltpu.VMEM((8, width), F32),
            pltpu.VMEM((NX * NC, own_rows, width), BF16),
            pltpu.VMEM((tok + ctxr, width), BF16),
            pltpu.VMEM((width, 768), BF16),
            pltpu.VMEM((NX * NC, 256, width), BF16),
            pltpu.VMEM((2, tok, 128), BF16),
            pltpu.VMEM((2, tok + ctxr, 128), BF16),
            pltpu.VMEM((2, tok + ctxr, 128), BF16),
            pltpu.VMEM((2, tok, 128), BF16),
            pltpu.VMEM((2, NZ, NY, tok + ctxr, 128), BF16),
            pltpu.VMEM((4 * tok, 128), BF16),
            pltpu.VMEM((4 * tok, 128), F32),
            pltpu.VMEM((4 * tok, 256), F32),
            pltpu.VMEM((2, block, NY * tok), F32),
            pltpu.VMEM((2, NX * NC, own_rows, 128), BF16),
            pltpu.VMEM((NX * NY, own_rows, 128), BF16),
            dma((6,)),
            dma((NZ - 1,)), dma((NZ - 1,)), dma((NY - 1,)), dma((NY - 1,)), dma((7,)), dma((7,)),
            dma((4,)), dma((4,)), dma((4,)), dma((4,)),
            dma((4,)), dma((4,)), dma((4,)), dma((4,)),
            dma((2,)), dma((2,)), dma((2,)), dma((2,)), dma((4,)),
            dma((2, 2)), dma((NZ, 2)), dma((NZ, 2)), dma((NZ, 2)), dma((NZ, 2)),
            dma((2, NX * NC)), dma((NX * NY,)),
        ],
        compiler_params=pltpu.CompilerParams(
            collective_id=0, has_side_effects=True, vmem_limit_bytes=60 * 2**20
        ),
    )(
        latent, context, lhs, shift_weight, scale_weight, gate_weight, extra, cos, sin,
        query_weight, key_weight, value_weight, out_weight,
    )


def solution(mesh):
    placed = (
        P(("sp", "tp"), None), P("sp", None), P(), P(),
        P("sp", "tp"), P("sp", "tp"), P("sp", "tp"),
        P(None, None, "tp"), P(None, None, "tp"), P(None, "tp"), P("tp", None), P("tp"), P("tp"),
    )
    return jax.shard_map(
        local, mesh=mesh, in_specs=placed, out_specs=P(("sp", "tp"), None), check_vma=False
    )
```

```python
import functools

import jax
import jax.numpy as jnp
import numpy as np
from jax import lax
from jax.experimental import pallas as pl
from jax.experimental.pallas import tpu as pltpu
from jax.sharding import PartitionSpec as P

HEAD_DIM = 64
GRID_W = 64
VALUE_DIM = 128
NX, NY, NZ, NC = 4, 4, 8, 2

norm_eps = 1e-06
rope_theta = 10000.0
log2_e = 1.4426950408889634

MESH = pl.DeviceIdType.MESH
F32, BF16 = jnp.float32, jnp.bfloat16
NT = (((1,), (1,)), ((), ()))


def send(src, dst, send_sem, recv_sem, device):
    pltpu.make_async_remote_copy(
        src_ref=src, dst_ref=dst, send_sem=send_sem, recv_sem=recv_sem,
        device_id=device, device_id_type=MESH,
    ).start()


def landed(ref, sem):
    pltpu.make_async_copy(ref, ref, sem).wait()


class Around:
    def __init__(self, buf, first, second, sems, x, c, place, split=False):
        self.split = split
        self.buf, self.first, self.second, self.place = buf, first, second, place
        self.send, self.recv, self.dsend, self.drecv = sems
        self.c = c
        self.x = x
        self.xl, self.xr, self.xa = (x + 3) % NX, (x + 1) % NX, (x + 2) % NX

    def at(self, x, c=None):
        return self.buf.at[x * NC + (self.c if c is None else c)]

    def start(self, src):
        own, other = self.at(self.x), self.place(self.x, 1 - self.c)
        send(src, own, self.send.at[0], self.recv.at[0], self.place(self.xr, self.c))
        send(src, own, self.send.at[1], self.recv.at[1], self.place(self.xl, self.c))
        send(src, own, self.dsend.at[0], self.drecv.at[0], other)

    def forward(self):
        left, right, other = self.at(self.xl), self.at(self.xr), self.place(self.x, 1 - self.c)
        landed(left, self.recv.at[0])
        a = self.first(left)
        send(a, a, self.send.at[2], self.recv.at[2], self.place(self.xr, self.c))
        landed(right, self.recv.at[1])
        b = self.second(right)
        send(b, b, self.send.at[3], self.recv.at[3], self.place(self.xl, self.c))
        if not self.split:
            send(left, left, self.dsend.at[1], self.drecv.at[1], other)
            send(right, right, self.dsend.at[2], self.drecv.at[2], other)

    def across(self, k):
        half, rest = self.buf.shape[1] // 2, k % 2
        piece = self.buf.at[((self.x + NX - 1 + 2 * (k // 2)) % NX) * NC + self.c, pl.ds(pl.multiple_of(rest * half, half), half)]
        send(piece, piece, self.dsend.at[4 + k], self.drecv.at[4 + k], self.place(self.x, 1 - self.c))

    def last(self):
        far, other = self.at(self.xa), self.place(self.x, 1 - self.c)
        landed(self.first(far), self.recv.at[2])
        landed(self.second(far), self.recv.at[3])
        send(far, far, self.dsend.at[3], self.drecv.at[3], other)

    def finish(self):
        for k, at in enumerate((self.x, self.xl, self.xr, self.xa)):
            if self.split and 0 < k < 3:
                half = self.buf.shape[1] // 2
                for j in range(2):
                    landed(self.at(at, 1 - self.c).at[pl.ds(j * half, half)], self.drecv.at[2 + 2 * k + j])
            else:
                landed(self.at(at, 1 - self.c), self.drecv.at[k])

    def drain(self, src):
        landed(src, self.send.at[0])
        landed(src, self.send.at[1])
        landed(src, self.dsend.at[0])
        landed(self.first(self.at(self.xl)), self.send.at[2])
        landed(self.second(self.at(self.xr)), self.send.at[3])
        for k, at in enumerate((self.xl, self.xr, self.xa), 1):
            if self.split and k < 3:
                half = self.buf.shape[1] // 2
                for j in range(2):
                    landed(self.at(at).at[pl.ds(j * half, half)], self.dsend.at[2 + 2 * k + j])
            else:
                landed(self.at(at), self.dsend.at[k])


def attend(qs, m, acc, k, v, sbuf, block, starts):
    n = len(starts)
    width = k.shape[0]
    v1 = jnp.concatenate([v, jnp.ones(v.shape, v.dtype)], axis=1)

    def scores(i):
        return lax.dot_general(qs[pl.ds(starts[i], block), :], k, NT, preferred_element_type=F32)

    sbuf[0, :, :width] = scores(0)
    for i in range(n):
        if i + 1 < n:
            sbuf[(i + 1) % 2, :, :width] = scores(i + 1)
        rows = pl.ds(starts[i], block)
        s = sbuf[i % 2, :, :width]
        before = m[rows, :]
        after = jnp.maximum(before, jnp.max(s, axis=1, keepdims=True))
        p = jnp.exp2(s - after[:, :1]).astype(BF16)
        rescale = jnp.exp2(before - after)
        m[rows, :] = after
        pv = jnp.dot(p, v1, preferred_element_type=F32)
        acc[rows, :] = acc[rows, :] * jnp.concatenate([rescale, rescale], axis=1) + pv


def kernel(
    tok, ctxr,
    lat_h, ctx_h, cl_h, cc_h, shw_h, scw_h, gaw_h, gain_h, lam_h, rowt_h, colt_h, wq, wk, wv, wo, out,
    lat, ctx, cond, modm, small, lam_s, rowt, colt, cos, sin,
    zbuf, ybuf, tbuf, modw, lbuf, hid, w, wall, qst, kst, vst, qbuf, kv, qs, m, acc, sbuf, obuf, hb,
    wsem, zs_s, zs_r, ys_s, ys_r, ts_s, ts_r,
    l_s, l_r, l_ds, l_dr, w_s, w_r, w_ds, w_dr,
    q_s, q_r, k_s, v_s, kv_r, own_s, fwd_s, ring_r, d_s, d_r, o_s, o_r,
):
    sp, tp = lax.axis_index("sp"), lax.axis_index("tp")
    z, y = sp // NY, sp % NY
    x, c = tp // NC, tp % NC

    def place(px, pc, py=None, pz=None):
        return ((z if pz is None else pz) * NY + (y if py is None else py), px * NC + pc)

    pairs = [
        (lat_h, lat), (cl_h, cond.at[pl.ds(0, 1)]), (cc_h, cond.at[pl.ds(1, 1)]),
        (shw_h, modm.at[0]), (scw_h, modm.at[1]), (gaw_h, modm.at[2]),
        (rowt_h, rowt), (colt_h, colt), (ctx_h, ctx), (gain_h, small), (lam_h, lam_s),
        (wk.at[0], w.at[:, pl.ds(256, 128)]), (wk.at[1], w.at[:, pl.ds(384, 128)]),
        (wv, w.at[:, pl.ds(512, 256)]),
        (wq.at[0], w.at[:, pl.ds(0, 128)]), (wq.at[1], w.at[:, pl.ds(128, 128)]),
        (wo, wall.at[tp]),
    ]
    loads = [pltpu.make_async_copy(src, dst, wsem.at[k]) for k, (src, dst) in enumerate(pairs)]

    barrier = pltpu.get_barrier_semaphore()
    others = [(dx, dy, dc) for dx in range(NX) for dy in range(NY) for dc in range(NC)][1:]
    for dz in range(1, NZ):
        pl.semaphore_signal(barrier, inc=1, device_id=place(x, c, pz=(z + dz) % NZ), device_id_type=MESH)
    for dx, dy, dc in others:
        pl.semaphore_signal(
            barrier, inc=1, device_id=place((x + dx) % NX, (c + dc) % NC, py=(y + dy) % NY), device_id_type=MESH
        )
    for load in loads:
        load.start()
    for load in loads[:6]:
        load.wait()

    span = modm.shape[1]
    v = cond[:, pl.ds(pl.multiple_of(sp // 2 * 128, 128), 128)]
    v = v / (1.0 + jnp.exp(-v))
    v = jnp.where(sp % 2 == 0, v, pltpu.roll(v, 128 - span, 1))[:, :span]
    row = lax.broadcasted_iota(jnp.int32, (16, span), 0)
    first, second, none = v[0:1], v[1:2], jnp.zeros((16, span), F32)

    def left(k):
        return jnp.where(row == k, first, jnp.where(row == k + 1, second, none)).astype(BF16)

    part = jnp.dot(left(0), modm[0], preferred_element_type=F32)
    part += jnp.dot(left(2), modm[1], preferred_element_type=F32)
    part += jnp.dot(jnp.where(row == 4, first, none).astype(BF16), modm[2], preferred_element_type=F32)
    zbuf[z] = part[:8]
    lbuf[tp] = lat[...]

    for load in loads[6:11]:
        load.wait()
    in_row = lax.broadcasted_iota(jnp.int32, (GRID_W, 128), 1) % 32 < 16
    for k in range(tok // GRID_W):
        r = sp * (tok // GRID_W) + k
        cos[k * GRID_W : (k + 1) * GRID_W, :] = jnp.where(in_row, rowt[0, pl.ds(r, 1), :], colt[0])
        sin[k * GRID_W : (k + 1) * GRID_W, :] = jnp.where(in_row, rowt[1, pl.ds(r, 1), :], colt[1])
    cos[tok : tok + ctxr, :] = jnp.ones((ctxr, 128), F32)
    sin[tok : tok + ctxr, :] = jnp.zeros((ctxr, 128), F32)
    lines = lax.broadcasted_iota(jnp.int32, (8, 256), 0)
    lane = lax.broadcasted_iota(jnp.int32, (8, 256), 1)
    lam = jnp.where(lane < VALUE_DIM, lam_s[0], lam_s[1])
    extra = jnp.where(lines == 5, small[...], jnp.where(lines == 6, lam, jnp.zeros((8, 256), F32)))

    pl.semaphore_wait(barrier, NZ - 1 + len(others))

    for d in range(1, NZ):
        send(zbuf.at[z], zbuf.at[z], zs_s.at[d - 1], zs_r.at[d - 1], place(x, c, pz=(z + d) % NZ))
    rows = Around(
        lbuf, lambda r: r.at[:, pl.ds(0, 1024)], lambda r: r.at[:, pl.ds(1024, 1024)], (l_s, l_r, l_ds, l_dr), x, c, place
    )
    rows.start(lat)
    for d in range(1, NZ):
        landed(zbuf.at[(z - d + NZ) % NZ], zs_r.at[d - 1])
    total = zbuf[0]
    for k in range(1, NZ):
        total += zbuf[k]
    ybuf[y] = total
    for d in range(1, NY):
        send(ybuf.at[y], ybuf.at[y], ys_s.at[d - 1], ys_r.at[d - 1], place(x, c, py=(y + d) % NY))
    for d in range(1, NY):
        landed(ybuf.at[(y - d + NY) % NY], ys_r.at[d - 1])
    tbuf[tp] = (ybuf[0] + ybuf[1]) + (ybuf[2] + ybuf[3]) + extra
    tps = [(dx, dc) for dx in range(NX) for dc in range(NC)][1:]
    for k, (dx, dc) in enumerate(tps):
        send(tbuf.at[tp], tbuf.at[tp], ts_s.at[k], ts_r.at[k], place((x + dx) % NX, (c + dc) % NC))
    rows.forward()
    for k, (dx, dc) in enumerate(tps):
        landed(tbuf.at[((x - dx + NX) % NX) * NC + (c + dc) % NC], ts_r.at[k])
    for k in range(NX * NC):
        modw[:, k * 256 : (k + 1) * 256] = tbuf[k]
    rows.last()

    loads[16].wait()
    weights = Around(
        wall, lambda r: r.at[pl.ds(0, 128)], lambda r: r.at[pl.ds(128, 128)], (w_s, w_r, w_ds, w_dr), x, c, place, True
    )
    weights.start(wall.at[tp])
    rows.finish()

    def modulate(values, shift, scale):
        values = values.astype(F32)
        inverse = lax.rsqrt(jnp.mean(values * values, axis=-1, keepdims=True) + norm_eps)
        return (values * inverse * (1.0 + scale) + shift).astype(BF16)

    own_rows = lat.shape[0]

    def one_block(k, _):
        hid[pl.ds(pl.multiple_of(k * own_rows, 16), own_rows), :] = modulate(lbuf[k], modw[0:1, :], modw[2:3, :])
        return 0

    lax.fori_loop(0, NX * NC, one_block, 0)
    hid[tok : tok + ctxr, :] = modulate(ctx[...], modw[1:2, :], modw[3:4, :])
    for load in loads[11:16]:
        load.wait()

    lane = lax.broadcasted_iota(jnp.int32, (tok + ctxr, 128), 1)
    low_half, low_head = lane % 64 < 32, lane < 64

    def turned(u):
        swapped = jnp.where(low_half, pltpu.roll(u, 96, 1), pltpu.roll(u, 32, 1))
        return u * cos[...] + swapped * sin[...]

    def by_head(both):
        m1, m2 = turned(both[:, :128]), turned(both[:, 128:])
        return (
            jnp.where(low_head, m1, pltpu.roll(m2, 64, 1)),
            jnp.where(low_head, pltpu.roll(m1, 64, 1), m2),
        )

    keys = by_head(jnp.dot(hid[...], w[:, 256:512], preferred_element_type=F32))
    kst[0], kst[1] = keys[0].astype(BF16), keys[1].astype(BF16)
    vals = jnp.dot(hid[...], w[:, 512:768], preferred_element_type=F32).astype(BF16)
    vst[0], vst[1] = vals[:, :128], vals[:, 128:]

    def self_head(j):
        return 2 * c + j == y

    for j in range(2):
        yd = 2 * c + j
        off = (y - yd + NY) % NY

        @pl.when(jnp.logical_or(yd != y, c != 0))
        def _():
            send(kst.at[j], kv.at[0, z, off], k_s.at[j], kv_r.at[off], place(x, 0, py=yd))

        @pl.when(jnp.logical_and(yd == y, c == 0))
        def _():
            kv[0, z, 0] = kst[j]

        @pl.when(jnp.logical_or(yd != y, c != 1))
        def _():
            send(vst.at[j], kv.at[1, z, off], v_s.at[j], kv_r.at[off], place(x, 1, py=yd))

        @pl.when(jnp.logical_and(yd == y, c == 1))
        def _():
            kv[1, z, 0] = vst[j]

    up, down, other = place(x, c, pz=(z + 1) % NZ), place(x, c, pz=(z + NZ - 1) % NZ), place(x, 1 - c)

    def own(o):
        if o == 0:

            @pl.when(c != y // 2)
            def _():
                landed(kv.at[c, z, 0], kv_r.at[0])
        else:
            landed(kv.at[c, z, o], kv_r.at[o])
        mine = kv.at[c, z, o]
        send(mine, mine, own_s.at[0, o], ring_r.at[0, 0, o], up)
        send(mine, mine, own_s.at[1, o], ring_r.at[1, 0, o], down)
        send(mine, mine, d_s.at[0, o], d_r.at[0, o], other)

    own(0)
    heads = by_head(jnp.dot(hid[...], w[:, 0:256], preferred_element_type=F32))
    for j in range(2):
        qst[j] = (heads[j][:tok] * (log2_e * HEAD_DIM**-0.5)).astype(BF16)
    for j in range(2):
        yd = 2 * c + j

        @pl.when(yd != y)
        def _():
            send(qst.at[j], qbuf.at[y % 2], q_s.at[j], q_r.at[y % 2], place(x, y // 2, py=yd))

        @pl.when(yd == y)
        def _():
            qbuf[y % 2] = qst[j]

    m[...] = jnp.full(m.shape, -jnp.inf, F32)
    acc[...] = jnp.zeros(acc.shape, F32)

    for o in (1, 3, 2):
        own(o)
    for i in range(2):

        @pl.when(2 * c + i != y)
        def _():
            landed(qbuf.at[i], q_r.at[i])

    low = lax.broadcasted_iota(jnp.int32, (tok, 128), 1) < 64
    for i in range(2):
        q = qbuf[i]
        nothing = jnp.zeros_like(q)
        qs[i * tok : (i + 1) * tok, :] = jnp.where(low, q, nothing)
        qs[(2 + i) * tok : (3 + i) * tok, :] = jnp.where(low, nothing, q)
    order = [k * tok + b for k in range(4) for b in range(0, tok, 128)]

    def places(u):
        far, p = (u + 1) // 2, (u + 1) % 2
        return far, p, p * ((u + 6) // 7), ((z - far + NZ) % NZ, (z + far) % NZ)

    def pass_on(u):
        far, p, _, froms = places(u)
        for q in range(2):
            o = 2 * p + q
            for side in range(2):
                piece = kv.at[c, froms[side], o]
                landed(piece, ring_r.at[side, far - 1, o])

                @pl.when(jnp.logical_or(far < 3, p == side))
                def _():
                    send(
                        piece, piece, fwd_s.at[side, far - 1, o], ring_r.at[side, far, o],
                        up if side == 0 else down,
                    )

                send(piece, piece, d_s.at[u, 2 * side + q], d_r.at[u, 2 * side + q], other)

    def unit(u, _):
        @pl.when(u < 6)
        def _():
            pass_on(u + 1)

        @pl.when(u == 3)
        def _():
            weights.forward()

        @pl.when(u >= 3)
        def _():
            weights.across(u - 3)

        _, p, first, froms = places(u)
        for q in range(2):
            landed(kv.at[1 - c, froms[0], 2 * first + q], d_r.at[u, q])
            landed(kv.at[1 - c, froms[1], 2 * p + q], d_r.at[u, 2 + q])
        k, v = (
            jnp.concatenate(
                [
                    kv[part, froms[0], pl.ds(2 * first, 2), 0:tok, :].reshape(2 * tok, 128),
                    kv[part, froms[1], pl.ds(2 * p, 2), 0:tok, :].reshape(2 * tok, 128),
                ]
            )
            for part in range(2)
        )
        attend(qs, m, acc, k, v, sbuf, 128, order)
        return 0

    lax.fori_loop(0, 6, unit, 0)

    def opposite_lands(q):
        for side in range(2):
            piece = kv.at[c, opposite, 2 * side + q]
            landed(piece, ring_r.at[side, 3, 2 * side + q])
            send(piece, piece, d_s.at[7, 2 * side + q], d_r.at[7, 2 * side + q], other)

    opposite = (z + NZ // 2) % NZ
    for q in range(2):
        landed(kv.at[1 - c, (z + 5) % NZ, 2 + q], d_r.at[6, q])
        landed(kv.at[1 - c, (z + 3) % NZ, 2 + q], d_r.at[6, 2 + q])
    k, v = (
        jnp.concatenate(
            [
                kv[part, (z + 5) % NZ, 2:4, 0:tok, :].reshape(2 * tok, 128),
                kv[part, (z + 3) % NZ, 2:4, 0:tok, :].reshape(2 * tok, 128),
            ]
            + [
                kv[part, (opposite + i) % NZ, :, tok : tok + ctxr, :].reshape(NY * ctxr, 128)
                for i in range(1, NZ)
            ]
        )
        for part in range(2)
    )
    opposite_lands(0)
    weights.across(3)
    attend(qs, m, acc, k, v, sbuf, 128, order)

    def finish(i):
        r1, r2 = pl.ds(i * tok, tok), pl.ds((2 + i) * tok, tok)
        mine = tbuf[2 * x + y // 2]
        picked = jnp.where(y % 2 == 0, mine[:, :128], mine[:, 128:])
        gain, factor = picked[5:6, :], picked[6:7, :]
        mixed = acc[r1, :128] / acc[r1, 128:] - factor * (acc[r2, :128] / acc[r2, 128:])
        normed = mixed * lax.rsqrt(jnp.mean(mixed * mixed, axis=-1, keepdims=True) + norm_eps) * gain
        obuf[i] = normed.astype(BF16).reshape(obuf.shape[1:])
        head = NY * x + y
        for t in range(NX * NC):
            home = jnp.logical_and(2 * c + i == y, tp == t)

            @pl.when(jnp.logical_not(home))
            def _():
                send(obuf.at[i, t], hb.at[head], o_s.at[i, t], o_r.at[head], (z * NY + 2 * c + i, t))

            @pl.when(home)
            def _():
                hb[head] = obuf[i, t]

    for q in range(2):
        if q == 0:
            opposite_lands(1)
            weights.last()
        for side in range(2):
            landed(kv.at[1 - c, opposite, 2 * side + q], d_r.at[7, 2 * side + q])
        k, v = (jnp.concatenate([kv[part, opposite, q], kv[part, opposite, 2 + q]]) for part in range(2))
        if q == 0:
            attend(qs, m, acc, k, v, sbuf, 128, order)
        else:
            for i in range(2):
                attend(qs, m, acc, k, v, sbuf, 128, [k2 * tok + b for k2 in (i, 2 + i) for b in range(0, tok, 128)])
                finish(i)
    weights.finish()
    for h in range(NX * NY):
        hx, hy = h // NY, h % NY

        @pl.when(jnp.logical_not(jnp.logical_and(jnp.logical_and(hx == x, hy == y), y // 2 == c)))
        def _():
            landed(hb.at[h], o_r.at[h])

    mixed_sum = jnp.zeros((own_rows, wall.shape[2]), F32)
    for g in range(NX * NC):
        pair = jnp.concatenate([hb[2 * g], hb[2 * g + 1]], axis=1)
        mixed_sum += jnp.dot(pair, wall[g], preferred_element_type=F32).astype(BF16).astype(F32)
    out[...] = modw[4:5, :] * mixed_sum

    for d in range(1, NZ):
        landed(zbuf.at[z], zs_s.at[d - 1])
    for d in range(1, NY):
        landed(ybuf.at[y], ys_s.at[d - 1])
    for k in range(len(tps)):
        landed(tbuf.at[tp], ts_s.at[k])
    rows.drain(lat)
    weights.drain(wall.at[tp])
    for j in range(2):
        yd = 2 * c + j

        @pl.when(yd != y)
        def _():
            landed(qst.at[j], q_s.at[j])

        @pl.when(jnp.logical_or(yd != y, c != 0))
        def _():
            landed(kst.at[j], k_s.at[j])

        @pl.when(jnp.logical_or(yd != y, c != 1))
        def _():
            landed(vst.at[j], v_s.at[j])

    for o in range(NY):
        for side in range(2):
            landed(kv.at[c, z, o], own_s.at[side, o])
            for far in range(3):
                if far < 2 or o // 2 == side:
                    landed(kv.at[c, z, o], fwd_s.at[side, far, o])
        for u in range(NZ):
            landed(kv.at[c, z, o], d_s.at[u, o])
    for i in range(2):
        for t in range(NX * NC):

            @pl.when(jnp.logical_not(jnp.logical_and(2 * c + i == y, tp == t)))
            def _():
                landed(obuf.at[i, t], o_s.at[i, t])


def tables(grid_rows):
    quarter = HEAD_DIM // 4
    inverse = np.float32(rope_theta) ** (-np.arange(quarter, dtype=np.float32) / np.float32(quarter))
    sign = np.array([-1.0, 1.0, -1.0, 1.0]).repeat(2 * quarter)

    def table(count):
        angles = (np.arange(count, dtype=np.float32)[:, None] * inverse).astype(np.float64)
        cos, sin = np.tile(np.cos(angles), (1, 8)), np.tile(np.sin(angles), (1, 8)) * sign
        return jnp.asarray(np.stack([cos, sin]).astype(np.float32))

    return table(grid_rows), table(GRID_W)


def local(
    latent, context, cond_latent, cond_context, shift_weight, scale_weight, gate_weight,
    query_weight, key_weight, value_weight, out_weight, lambda_heads, out_gain,
):
    own_rows, width = latent.shape
    ctxr = context.shape[0]
    tok = own_rows * NX * NC
    rowt, colt = tables(tok * lax.axis_size("sp") // GRID_W)
    hbm = pl.BlockSpec(memory_space=pl.ANY)
    dma = pltpu.SemaphoreType.DMA
    gated = pl.pallas_call(
        functools.partial(kernel, tok, ctxr),
        out_shape=jax.ShapeDtypeStruct((own_rows, width), F32),
        in_specs=[hbm] * 15,
        out_specs=pl.BlockSpec(memory_space=pltpu.VMEM),
        scratch_shapes=[
            pltpu.VMEM((own_rows, width), BF16),
            pltpu.VMEM((ctxr, width), BF16),
            pltpu.VMEM((2, width), F32),
            pltpu.VMEM((3, *shift_weight.shape), BF16),
            pltpu.VMEM((1, 256), F32),
            pltpu.SMEM(lambda_heads.shape, F32),
            pltpu.VMEM(rowt.shape, F32),
            pltpu.VMEM(colt.shape, F32),
            pltpu.VMEM((tok + ctxr, 128), F32),
            pltpu.VMEM((tok + ctxr, 128), F32),
            pltpu.VMEM((NZ, 8, 256), F32),
            pltpu.VMEM((NY, 8, 256), F32),
            pltpu.VMEM((NX * NC, 8, 256), F32),
            pltpu.VMEM((8, width), F32),
            pltpu.VMEM((NX * NC, own_rows, width), BF16),
            pltpu.VMEM((tok + ctxr, width), BF16),
            pltpu.VMEM((width, 768), BF16),
            pltpu.VMEM((NX * NC, 256, width), BF16),
            pltpu.VMEM((2, tok, 128), BF16),
            pltpu.VMEM((2, tok + ctxr, 128), BF16),
            pltpu.VMEM((2, tok + ctxr, 128), BF16),
            pltpu.VMEM((2, tok, 128), BF16),
            pltpu.VMEM((2, NZ, NY, tok + ctxr, 128), BF16),
            pltpu.VMEM((4 * tok, 128), BF16),
            pltpu.VMEM((4 * tok, 128), F32),
            pltpu.VMEM((4 * tok, 256), F32),
            pltpu.VMEM((2, 128, NY * tok + (NZ - 1) * NY * ctxr), F32),
            pltpu.VMEM((2, NX * NC, own_rows, 128), BF16),
            pltpu.VMEM((NX * NY, own_rows, 128), BF16),
            dma((17,)),
            dma((NZ - 1,)), dma((NZ - 1,)), dma((NY - 1,)), dma((NY - 1,)), dma((7,)), dma((7,)),
            dma((4,)), dma((4,)), dma((4,)), dma((4,)),
            dma((4,)), dma((4,)), dma((8,)), dma((8,)),
            dma((2,)), dma((2,)), dma((2,)), dma((2,)), dma((NY,)),
            dma((2, NY)), dma((2, 3, NY)), dma((2, 4, NY)), dma((NZ, NY)), dma((NZ, NY)),
            dma((2, NX * NC)), dma((NX * NY,)),
        ],
        compiler_params=pltpu.CompilerParams(
            collective_id=0, has_side_effects=True, vmem_limit_bytes=60 * 2**20
        ),
    )(
        latent, context, cond_latent[None], cond_context[None], shift_weight, scale_weight, gate_weight,
        out_gain[None], lambda_heads, rowt, colt, query_weight, key_weight, value_weight, out_weight,
    )
    return (latent.astype(F32) + gated).astype(BF16)


def solution(mesh):
    placed = (
        P(("sp", "tp"), None), P("sp", None), P(), P(),
        P("sp", "tp"), P("sp", "tp"), P("sp", "tp"),
        P(None, None, "tp"), P(None, None, "tp"), P(None, "tp"), P("tp", None), P("tp"), P("tp"),
    )
    return jax.shard_map(
        local, mesh=mesh, in_specs=placed, out_specs=P(("sp", "tp"), None), check_vma=False
    )
```

```python
import functools

import jax
import jax.numpy as jnp
import numpy as np
from jax import lax
from jax.experimental import pallas as pl
from jax.experimental.pallas import tpu as pltpu
from jax.sharding import PartitionSpec as P

HEAD_DIM = 64
GRID_W = 64
VALUE_DIM = 128
NX, NY, NZ, NC = 4, 4, 8, 2

norm_eps = 1e-06
rope_theta = 10000.0
log2_e = 1.4426950408889634

MESH = pl.DeviceIdType.MESH
F32, BF16 = jnp.float32, jnp.bfloat16
NT = (((1,), (1,)), ((), ()))


def send(src, dst, send_sem, recv_sem, device):
    pltpu.make_async_remote_copy(
        src_ref=src, dst_ref=dst, send_sem=send_sem, recv_sem=recv_sem,
        device_id=device, device_id_type=MESH,
    ).start()


def landed(ref, sem):
    pltpu.make_async_copy(ref, ref, sem).wait()


class Around:
    def __init__(self, buf, first, second, sems, x, c, place, split=False):
        self.split = split
        self.buf, self.first, self.second, self.place = buf, first, second, place
        self.sent, self.recv, self.drecv = sems
        self.c = c
        self.x = x
        self.xl, self.xr, self.xa = (x + 3) % NX, (x + 1) % NX, (x + 2) % NX

    def at(self, x, c=None):
        return self.buf.at[x * NC + (self.c if c is None else c)]

    def start(self, src):
        own, other = self.at(self.x), self.place(self.x, 1 - self.c)
        send(src, own, self.sent, self.recv.at[0], self.place(self.xr, self.c))
        send(src, own, self.sent, self.recv.at[1], self.place(self.xl, self.c))
        send(src, own, self.sent, self.drecv.at[0], other)

    def forward(self):
        left, right = self.at(self.xl), self.at(self.xr)
        landed(left, self.recv.at[0])
        a = self.first(left)
        send(a, a, self.sent, self.recv.at[2], self.place(self.xr, self.c))
        landed(right, self.recv.at[1])
        b = self.second(right)
        send(b, b, self.sent, self.recv.at[3], self.place(self.xl, self.c))

    def near(self):
        left, right, other = self.at(self.xl), self.at(self.xr), self.place(self.x, 1 - self.c)
        send(left, left, self.sent, self.drecv.at[1], other)
        send(right, right, self.sent, self.drecv.at[2], other)

    def across(self, k):
        half, rest = self.buf.shape[1] // 2, k % 2
        piece = self.buf.at[((self.x + NX - 1 + 2 * (k // 2)) % NX) * NC + self.c, pl.ds(pl.multiple_of(rest * half, half), half)]
        send(piece, piece, self.sent, self.drecv.at[4 + k], self.place(self.x, 1 - self.c))

    def last(self):
        far, other = self.at(self.xa), self.place(self.x, 1 - self.c)
        landed(self.first(far), self.recv.at[2])
        landed(self.second(far), self.recv.at[3])
        send(far, far, self.sent, self.drecv.at[3], other)

    def finish(self):
        for k, at in enumerate((self.x, self.xl, self.xr, self.xa)):
            if self.split and 0 < k < 3:
                half = self.buf.shape[1] // 2
                for j in range(2):
                    landed(self.at(at, 1 - self.c).at[pl.ds(j * half, half)], self.drecv.at[2 + 2 * k + j])
            else:
                landed(self.at(at, 1 - self.c), self.drecv.at[k])

    def drain(self):
        landed(self.buf.at[pl.ds(0, 7)], self.sent)


def attend(qs, m, acc, k, v, sbuf, block, starts):
    n = len(starts)
    width = k.shape[0]
    v1 = jnp.concatenate([v, jnp.ones(v.shape, v.dtype)], axis=1)

    def scores(i):
        return lax.dot_general(qs[pl.ds(starts[i], block), :], k, NT, preferred_element_type=F32)

    sbuf[0, :, :width] = scores(0)
    for i in range(n):
        if i + 1 < n:
            sbuf[(i + 1) % 2, :, :width] = scores(i + 1)
        rows = pl.ds(starts[i], block)
        s = sbuf[i % 2, :, :width]
        before = m[rows, :]
        after = jnp.maximum(before, jnp.max(s, axis=1, keepdims=True))
        p = jnp.exp2(s - after[:, :1]).astype(BF16)
        rescale = jnp.exp2(before - after)
        m[rows, :] = after
        pv = jnp.dot(p, v1, preferred_element_type=F32)
        acc[rows, :] = acc[rows, :] * jnp.concatenate([rescale, rescale], axis=1) + pv


def kernel(
    tok, ctxr,
    lat_h, ctx_h, cl_h, cc_h, shw_h, scw_h, gaw_h, gain_h, lam_h, rowt_h, colt_h, wq, wk, wv, wo, out,
    lat, ctx, cond, modm, small, lam_s, rowt, colt, cos, sin,
    zbuf, ybuf, tbuf, modw, inv, lbuf, hid, w, wall, qst, kst, vst, qbuf, kv, qs, m, acc, sbuf, obuf, hb,
    wsem, vec_s, vec_r, gather_s, l_r, l_dr, w_r, w_dr,
    q_s, q_r, k_s, v_s, kv_r, kv_s, ring_r, d_r, o_s, o_r,
):
    sp, tp = lax.axis_index("sp"), lax.axis_index("tp")
    z, y = sp // NY, sp % NY
    x, c = tp // NC, tp % NC

    def place(px, pc, py=None, pz=None):
        return ((z if pz is None else pz) * NY + (y if py is None else py), px * NC + pc)

    pairs = [
        (lat_h, lat), (cl_h, cond.at[pl.ds(0, 1)]), (cc_h, cond.at[pl.ds(1, 1)]),
        (shw_h, modm.at[0]), (scw_h, modm.at[1]), (gaw_h, modm.at[2]),
        (rowt_h, rowt), (colt_h, colt), (ctx_h, ctx), (gain_h, small), (lam_h, lam_s),
        (wk.at[0], w.at[:, pl.ds(256, 128)]), (wk.at[1], w.at[:, pl.ds(384, 128)]),
        (wv, w.at[:, pl.ds(512, 256)]),
        (wq.at[0], w.at[:, pl.ds(0, 128)]), (wq.at[1], w.at[:, pl.ds(128, 128)]),
        (wo, wall.at[tp]),
    ]
    group = [0, 1, 1, 2, 2, 2, 3, 4, 5, 6, 7, 8, 8, 8, 8, 8, 9]
    loads = [pltpu.make_async_copy(src, dst, wsem.at[group[k]]) for k, (src, dst) in enumerate(pairs)]

    barrier = pltpu.get_barrier_semaphore()
    others = [(dx, dy, dc) for dx in range(NX) for dy in range(NY) for dc in range(NC)][1:]
    for dz in range(1, NZ):
        pl.semaphore_signal(barrier, inc=1, device_id=place(x, c, pz=(z + dz) % NZ), device_id_type=MESH)
    for dx, dy, dc in others:
        pl.semaphore_signal(
            barrier, inc=1, device_id=place((x + dx) % NX, (c + dc) % NC, py=(y + dy) % NY), device_id_type=MESH
        )
    for load in loads:
        load.start()
    landed(lat, wsem.at[0])
    landed(cond, wsem.at[1])
    landed(modm, wsem.at[2])

    span = modm.shape[1]
    v = cond[:, pl.ds(pl.multiple_of(sp // 2 * 128, 128), 128)]
    v = v / (1.0 + jnp.exp(-v))
    v = jnp.where(sp % 2 == 0, v, pltpu.roll(v, 128 - span, 1))[:, :span]
    row = lax.broadcasted_iota(jnp.int32, (16, span), 0)
    first, second, none = v[0:1], v[1:2], jnp.zeros((16, span), F32)

    def left(k):
        return jnp.where(row == k, first, jnp.where(row == k + 1, second, none)).astype(BF16)

    part = jnp.dot(left(0), modm[0], preferred_element_type=F32)
    part += jnp.dot(left(2), modm[1], preferred_element_type=F32)
    part += jnp.dot(jnp.where(row == 4, first, none).astype(BF16), modm[2], preferred_element_type=F32)
    zbuf[0] = part[:8]
    lbuf[tp] = lat[...]

    for load in loads[6:11]:
        load.wait()
    in_row = lax.broadcasted_iota(jnp.int32, (GRID_W, 128), 1) % 32 < 16
    for k in range(tok // GRID_W):
        r = sp * (tok // GRID_W) + k
        cos[k * GRID_W : (k + 1) * GRID_W, :] = jnp.where(in_row, rowt[0, pl.ds(r, 1), :], colt[0])
        sin[k * GRID_W : (k + 1) * GRID_W, :] = jnp.where(in_row, rowt[1, pl.ds(r, 1), :], colt[1])
    cos[tok : tok + ctxr, :] = jnp.ones((ctxr, 128), F32)
    sin[tok : tok + ctxr, :] = jnp.zeros((ctxr, 128), F32)
    lines = lax.broadcasted_iota(jnp.int32, (8, 256), 0)
    lane = lax.broadcasted_iota(jnp.int32, (8, 256), 1)
    lam = jnp.where(lane < VALUE_DIM, lam_s[0], lam_s[1])
    extra = jnp.where(lines == 5, small[...], jnp.where(lines == 6, lam, jnp.zeros((8, 256), F32)))

    pl.semaphore_wait(barrier, NZ - 1 + len(others))

    for d in range(1, NZ):
        send(zbuf.at[0], zbuf.at[d], vec_s.at[0], vec_r.at[0], place(x, c, pz=(z + d) % NZ))
    rows = Around(
        lbuf, lambda r: r.at[:, pl.ds(0, 1024)], lambda r: r.at[:, pl.ds(1024, 1024)], (gather_s.at[0], l_r, l_dr), x, c, place
    )
    rows.start(lat)
    landed(zbuf.at[pl.ds(1, NZ - 1)], vec_r.at[0])
    total = zbuf[0]
    for k in range(1, NZ):
        total += zbuf[k]
    ybuf[0] = total
    for d in range(1, NY):
        send(ybuf.at[0], ybuf.at[d], vec_s.at[1], vec_r.at[1], place(x, c, py=(y + d) % NY))
    rows.forward()
    landed(ybuf.at[pl.ds(1, NY - 1)], vec_r.at[1])
    tbuf[tp] = (ybuf[0] + ybuf[1]) + (ybuf[2] + ybuf[3]) + extra
    tps = [(dx, dc) for dx in range(NX) for dc in range(NC)][1:]
    for k, (dx, dc) in enumerate(tps):
        send(tbuf.at[tp], tbuf.at[tp], vec_s.at[2], vec_r.at[2 + k], place((x + dx) % NX, (c + dc) % NC))
    rows.near()
    rows.last()
    loads[16].wait()
    weights = Around(
        wall, lambda r: r.at[pl.ds(0, 128)], lambda r: r.at[pl.ds(128, 128)], (gather_s.at[1], w_r, w_dr), x, c, place, True
    )
    weights.start(wall.at[tp])
    rows.finish()

    def inverse_of(values):
        values = values.astype(F32)
        return lax.rsqrt(jnp.mean(values * values, axis=-1, keepdims=True) + norm_eps)

    def modulate(values, inverse, shift, scale):
        return (values.astype(F32) * inverse * (1.0 + scale) + shift).astype(BF16)

    own_rows = lat.shape[0]

    def one_inverse(k, _):
        rows_of = pl.ds(pl.multiple_of(k * own_rows, 16), own_rows)
        inv[rows_of, :] = jnp.broadcast_to(inverse_of(lbuf[k]), (own_rows, 128))
        return 0

    lax.fori_loop(0, NX * NC, one_inverse, 0)
    inv[tok : tok + ctxr, :] = jnp.broadcast_to(inverse_of(ctx[...]), (ctxr, 128))
    for k, (dx, dc) in enumerate(tps):
        landed(tbuf.at[((x - dx + NX) % NX) * NC + (c + dc) % NC], vec_r.at[2 + k])
    for k in range(NX * NC):
        modw[:, k * 256 : (k + 1) * 256] = tbuf[k]

    def one_block(k, _):
        rows_of = pl.ds(pl.multiple_of(k * own_rows, 16), own_rows)
        hid[rows_of, :] = modulate(lbuf[k], inv[rows_of, :][:, :1], modw[0:1, :], modw[2:3, :])
        return 0

    lax.fori_loop(0, NX * NC, one_block, 0)
    hid[tok : tok + ctxr, :] = modulate(ctx[...], inv[tok : tok + ctxr, :][:, :1], modw[1:2, :], modw[3:4, :])
    landed(w, wsem.at[8])

    lane = lax.broadcasted_iota(jnp.int32, (tok + ctxr, 128), 1)
    low_half, low_head = lane % 64 < 32, lane < 64

    def turned(u):
        swapped = jnp.where(low_half, pltpu.roll(u, 96, 1), pltpu.roll(u, 32, 1))
        return u * cos[...] + swapped * sin[...]

    def by_head(both):
        m1, m2 = turned(both[:, :128]), turned(both[:, 128:])
        return (
            jnp.where(low_head, m1, pltpu.roll(m2, 64, 1)),
            jnp.where(low_head, pltpu.roll(m1, 64, 1), m2),
        )

    near, rest = (y + 1) % 2, y % 2
    ynear, yrest = 2 * c + near, 2 * c + rest
    here = yrest == y

    def to_near(stage, sems, part):
        off = (y - ynear + NY) % NY
        send(stage.at[near], kv.at[part, z, off], sems.at[0], kv_r.at[off], place(x, part, py=ynear))

        @pl.when(jnp.logical_and(here, c == part))
        def _():
            kv[part, z, 0] = stage[rest]

        @pl.when(jnp.logical_and(here, c != part))
        def _():
            send(stage.at[rest], kv.at[part, z, 0], sems.at[1], kv_r.at[0], place(x, part))

    def to_far(stage, sems, part):
        @pl.when(jnp.logical_not(here))
        def _():
            send(stage.at[rest], kv.at[part, z, 2], sems.at[1], kv_r.at[2], place(x, part, py=yrest))

    vals = jnp.dot(hid[...], w[:, 512:768], preferred_element_type=F32).astype(BF16)
    vst[0], vst[1] = vals[:, :128], vals[:, 128:]
    to_near(vst, v_s, 1)
    keys = by_head(jnp.dot(hid[...], w[:, 256:512], preferred_element_type=F32))
    kst[0], kst[1] = keys[0].astype(BF16), keys[1].astype(BF16)
    to_near(kst, k_s, 0)
    to_far(vst, v_s, 1)
    to_far(kst, k_s, 0)

    up, down, other = place(x, c, pz=(z + 1) % NZ), place(x, c, pz=(z + NZ - 1) % NZ), place(x, 1 - c)

    def own(o):
        if o == 0:

            @pl.when(c != y // 2)
            def _():
                landed(kv.at[c, z, 0], kv_r.at[0])
        else:
            landed(kv.at[c, z, o], kv_r.at[o])
        mine = kv.at[c, z, o]
        send(mine, mine, kv_s.at[0], ring_r.at[0, 0, o], up)
        send(mine, mine, kv_s.at[0], ring_r.at[1, 0, o], down)
        send(mine, mine, kv_s.at[2], d_r.at[0, o // 2], other)

    own(0)
    heads = by_head(jnp.dot(hid[...], w[:, 0:256], preferred_element_type=F32))
    for j in range(2):
        qst[j] = (heads[j][:tok] * (log2_e * HEAD_DIM**-0.5)).astype(BF16)
    send(qst.at[near], qbuf.at[y % 2], q_s.at[0], q_r.at[y % 2], place(x, y // 2, py=ynear))

    @pl.when(here)
    def _():
        qbuf[y % 2] = qst[rest]

    @pl.when(jnp.logical_not(here))
    def _():
        send(qst.at[rest], qbuf.at[y % 2], q_s.at[1], q_r.at[y % 2], place(x, y // 2, py=yrest))

    m[...] = jnp.full(m.shape, -jnp.inf, F32)
    acc[...] = jnp.zeros(acc.shape, F32)
    for o in (1, 3, 2):
        own(o)
    for i in range(2):

        @pl.when(2 * c + i != y)
        def _():
            landed(qbuf.at[i], q_r.at[i])

    low = lax.broadcasted_iota(jnp.int32, (tok, 128), 1) < 64
    for i in range(2):
        q = qbuf[i]
        nothing = jnp.zeros_like(q)
        qs[i * tok : (i + 1) * tok, :] = jnp.where(low, q, nothing)
        qs[(2 + i) * tok : (3 + i) * tok, :] = jnp.where(low, nothing, q)
    order = [k * tok + b for k in range(4) for b in range(0, tok, 128)]

    def places(u):
        far, p = (u + 1) // 2, (u + 1) % 2
        return far, p, p * ((u + 6) // 7), ((z - far + NZ) % NZ, (z + far) % NZ)

    def pass_on(u, q):
        far, p, _, froms = places(u)
        o = 2 * p + q
        for side in range(2):
            piece = kv.at[c, froms[side], o]
            landed(piece, ring_r.at[side, far - 1, o])

            @pl.when(jnp.logical_or(far < 3, c == side))
            def _():
                send(piece, piece, kv_s.at[1], ring_r.at[side, far, o], up if side == 0 else down)

            send(piece, piece, kv_s.at[2], d_r.at[u, side], other)

    opposite = (z + NZ // 2) % NZ

    def opposite_lands(p):
        for o in (2 * p, 2 * p + 1):
            piece = kv.at[c, opposite, o]
            landed(piece, ring_r.at[c, 3, o])
            send(piece, piece, kv_s.at[2], d_r.at[7, p], other)

    def unit(u, _):
        @pl.when(u < 6)
        def _():
            pass_on(u + 1, 0)

        @pl.when(u == 6)
        def _():
            opposite_lands(0)

        _, p, first, froms = places(u)
        landed(kv.at[1 - c, froms[0], pl.ds(2 * first, 2)], d_r.at[u, 0])
        landed(kv.at[1 - c, froms[1], pl.ds(2 * p, 2)], d_r.at[u, 1])
        k, v = (
            jnp.concatenate(
                [
                    kv[part, froms[0], pl.ds(2 * first, 2), 0:tok, :].reshape(2 * tok, 128),
                    kv[part, froms[1], pl.ds(2 * p, 2), 0:tok, :].reshape(2 * tok, 128),
                ]
            )
            for part in range(2)
        )
        attend(qs, m, acc, k, v, sbuf, 128, order[:6])
        @pl.when(u < 6)
        def _():
            pass_on(u + 1, 1)

        @pl.when(u == 6)
        def _():
            opposite_lands(1)

        @pl.when(u == 3)
        def _():
            weights.forward()

        @pl.when(u >= 3)
        def _():
            weights.across(u - 3)

        attend(qs, m, acc, k, v, sbuf, 128, order[6:])
        return 0

    lax.fori_loop(0, 7, unit, 0)

    def finish(i):
        r1, r2 = pl.ds(i * tok, tok), pl.ds((2 + i) * tok, tok)
        mine = tbuf[2 * x + y // 2]
        picked = jnp.where(y % 2 == 0, mine[:, :128], mine[:, 128:])
        gain, factor = picked[5:6, :], picked[6:7, :]
        mixed = acc[r1, :128] / acc[r1, 128:] - factor * (acc[r2, :128] / acc[r2, 128:])
        normed = mixed * lax.rsqrt(jnp.mean(mixed * mixed, axis=-1, keepdims=True) + norm_eps) * gain
        obuf[i] = normed.astype(BF16).reshape(obuf.shape[1:])
        head = NY * x + y
        for t in range(NX * NC):
            home = jnp.logical_and(2 * c + i == y, tp == t)

            @pl.when(jnp.logical_not(home))
            def _():
                send(obuf.at[i, t], hb.at[head], o_s.at[0], o_r.at[head // 2], (z * NY + 2 * c + i, t))

            @pl.when(home)
            def _():
                hb[head] = obuf[i, t]

    for p in range(2):
        landed(kv.at[1 - c, opposite, pl.ds(2 * p, 2)], d_r.at[7, p])
    k, v = (
        jnp.concatenate(
            [
                kv[part, opposite, :, 0:tok, :].reshape(NY * tok, 128),
                kv[part, :, :, tok : tok + ctxr, :].reshape(NZ * NY * ctxr, 128),
            ]
        )
        for part in range(2)
    )
    for i in range(2):
        attend(qs, m, acc, k, v, sbuf, 128, [k2 * tok + b for k2 in (i, 2 + i) for b in range(0, tok, 128)])
        finish(i)
        if i == 0:
            weights.last()
    weights.finish()
    mixed_sum = jnp.zeros((own_rows, wall.shape[2]), F32)
    for dx in (0, 1, 3, 2):
        hx = (x + dx) % NX
        for half in range(2):
            g = 2 * hx + half
            if dx == 0:

                @pl.when(jnp.logical_and(c == half, y // 2 == half))
                def _():
                    landed(hb.at[2 * g + 1 - y % 2], o_r.at[g])

                @pl.when(jnp.logical_not(jnp.logical_and(c == half, y // 2 == half)))
                def _():
                    landed(hb.at[pl.ds(2 * g, 2)], o_r.at[g])
            else:
                landed(hb.at[pl.ds(2 * g, 2)], o_r.at[g])
            pair = jnp.concatenate([hb[2 * g], hb[2 * g + 1]], axis=1)
            mixed_sum += jnp.dot(pair, wall[g], preferred_element_type=F32).astype(BF16).astype(F32)
    out[...] = (lat[...].astype(F32) + modw[4:5, :] * mixed_sum).astype(BF16)

    landed(zbuf.at[pl.ds(0, NZ - 1)], vec_s.at[0])
    landed(ybuf.at[pl.ds(0, NY - 1)], vec_s.at[1])
    landed(tbuf.at[pl.ds(0, len(tps))], vec_s.at[2])
    rows.drain()
    weights.drain()
    landed(qst.at[0], q_s.at[0])
    landed(kst.at[0], k_s.at[0])
    landed(vst.at[0], v_s.at[0])

    @pl.when(jnp.logical_not(here))
    def _():
        landed(qst.at[1], q_s.at[1])

    @pl.when(jnp.logical_or(jnp.logical_not(here), c != 0))
    def _():
        landed(kst.at[1], k_s.at[1])

    @pl.when(jnp.logical_or(jnp.logical_not(here), c != 1))
    def _():
        landed(vst.at[1], v_s.at[1])

    landed(kv.at[c, pl.ds(0, 2)], kv_s.at[0])
    landed(kv.at[c, pl.ds(0, 5)], kv_s.at[1])
    landed(kv.at[c], kv_s.at[2])

    @pl.when(c == y // 2)
    def _():
        landed(hb.at[pl.ds(0, NX * NY - 1)], o_s.at[0])

    @pl.when(c != y // 2)
    def _():
        landed(hb, o_s.at[0])


def tables(grid_rows):
    quarter = HEAD_DIM // 4
    inverse = np.float32(rope_theta) ** (-np.arange(quarter, dtype=np.float32) / np.float32(quarter))
    sign = np.array([-1.0, 1.0, -1.0, 1.0]).repeat(2 * quarter)

    def table(count):
        angles = (np.arange(count, dtype=np.float32)[:, None] * inverse).astype(np.float64)
        cos, sin = np.tile(np.cos(angles), (1, 8)), np.tile(np.sin(angles), (1, 8)) * sign
        return jnp.asarray(np.stack([cos, sin]).astype(np.float32))

    return table(grid_rows), table(GRID_W)


def local(
    latent, context, cond_latent, cond_context, shift_weight, scale_weight, gate_weight,
    query_weight, key_weight, value_weight, out_weight, lambda_heads, out_gain,
):
    own_rows, width = latent.shape
    ctxr = context.shape[0]
    tok = own_rows * NX * NC
    rowt, colt = tables(tok * lax.axis_size("sp") // GRID_W)
    hbm = pl.BlockSpec(memory_space=pl.ANY)
    dma = pltpu.SemaphoreType.DMA
    return pl.pallas_call(
        functools.partial(kernel, tok, ctxr),
        out_shape=jax.ShapeDtypeStruct((own_rows, width), BF16),
        in_specs=[hbm] * 15,
        out_specs=pl.BlockSpec(memory_space=pltpu.VMEM),
        scratch_shapes=[
            pltpu.VMEM((own_rows, width), BF16),
            pltpu.VMEM((ctxr, width), BF16),
            pltpu.VMEM((2, width), F32),
            pltpu.VMEM((3, *shift_weight.shape), BF16),
            pltpu.VMEM((1, 256), F32),
            pltpu.SMEM(lambda_heads.shape, F32),
            pltpu.VMEM(rowt.shape, F32),
            pltpu.VMEM(colt.shape, F32),
            pltpu.VMEM((tok + ctxr, 128), F32),
            pltpu.VMEM((tok + ctxr, 128), F32),
            pltpu.VMEM((NZ, 8, 256), F32),
            pltpu.VMEM((NY, 8, 256), F32),
            pltpu.VMEM((NX * NC, 8, 256), F32),
            pltpu.VMEM((8, width), F32),
            pltpu.VMEM((tok + ctxr, 128), F32),
            pltpu.VMEM((NX * NC, own_rows, width), BF16),
            pltpu.VMEM((tok + ctxr, width), BF16),
            pltpu.VMEM((width, 768), BF16),
            pltpu.VMEM((NX * NC, 256, width), BF16),
            pltpu.VMEM((2, tok, 128), BF16),
            pltpu.VMEM((2, tok + ctxr, 128), BF16),
            pltpu.VMEM((2, tok + ctxr, 128), BF16),
            pltpu.VMEM((2, tok, 128), BF16),
            pltpu.VMEM((2, NZ, NY, tok + ctxr, 128), BF16),
            pltpu.VMEM((4 * tok, 128), BF16),
            pltpu.VMEM((4 * tok, 128), F32),
            pltpu.VMEM((4 * tok, 256), F32),
            pltpu.VMEM((2, 128, NY * (tok + NZ * ctxr)), F32),
            pltpu.VMEM((2, NX * NC, own_rows, 128), BF16),
            pltpu.VMEM((NX * NY, own_rows, 128), BF16),
            dma((10,)), dma((3,)), dma((9,)), dma((2,)), dma((4,)), dma((4,)), dma((4,)), dma((8,)),
            dma((2,)), dma((2,)), dma((2,)), dma((2,)), dma((NY,)),
            dma((3,)), dma((2, 4, NY)), dma((NZ, 2)), dma((1,)), dma((NX * NC,)),
        ],
        compiler_params=pltpu.CompilerParams(
            collective_id=0, has_side_effects=True, vmem_limit_bytes=60 * 2**20
        ),
    )(
        latent, context, cond_latent[None], cond_context[None], shift_weight, scale_weight, gate_weight,
        out_gain[None], lambda_heads, rowt, colt, query_weight, key_weight, value_weight, out_weight,
    )


def solution(mesh):
    placed = (
        P(("sp", "tp"), None), P("sp", None), P(), P(),
        P("sp", "tp"), P("sp", "tp"), P("sp", "tp"),
        P(None, None, "tp"), P(None, None, "tp"), P(None, "tp"), P("tp", None), P("tp"), P("tp"),
    )
    return jax.shard_map(
        local, mesh=mesh, in_specs=placed, out_specs=P(("sp", "tp"), None), check_vma=False
    )
```

```python
import functools

import jax
import jax.numpy as jnp
import numpy as np
from jax import lax
from jax.experimental import pallas as pl
from jax.experimental.pallas import tpu as pltpu
from jax.sharding import PartitionSpec as P

HEAD_DIM = 64
GRID_W = 64
VALUE_DIM = 128
NX, NY, NZ, NC = 4, 4, 8, 2

norm_eps = 1e-06
rope_theta = 10000.0
log2_e = 1.4426950408889634

MESH = pl.DeviceIdType.MESH
F32, BF16 = jnp.float32, jnp.bfloat16
NT = (((1,), (1,)), ((), ()))


def send(src, dst, send_sem, recv_sem, device):
    pltpu.make_async_remote_copy(
        src_ref=src, dst_ref=dst, send_sem=send_sem, recv_sem=recv_sem,
        device_id=device, device_id_type=MESH,
    ).start()


def landed(ref, sem):
    pltpu.make_async_copy(ref, ref, sem).wait()


class Around:
    def __init__(self, buf, first, second, sems, x, c, place, split=False):
        self.split = split
        self.buf, self.first, self.second, self.place = buf, first, second, place
        self.sent, self.recv, self.drecv = sems
        self.c = c
        self.x = x
        self.xl, self.xr, self.xa = (x + 3) % NX, (x + 1) % NX, (x + 2) % NX

    def at(self, x, c=None):
        return self.buf.at[x * NC + (self.c if c is None else c)]

    def start(self, src):
        own, other = self.at(self.x), self.place(self.x, 1 - self.c)
        send(src, own, self.sent, self.recv.at[0], self.place(self.xr, self.c))
        send(src, own, self.sent, self.recv.at[1], self.place(self.xl, self.c))
        send(src, own, self.sent, self.drecv.at[0], other)

    def forward(self):
        left, right = self.at(self.xl), self.at(self.xr)
        landed(left, self.recv.at[0])
        a = self.first(left)
        send(a, a, self.sent, self.recv.at[2], self.place(self.xr, self.c))
        landed(right, self.recv.at[1])
        b = self.second(right)
        send(b, b, self.sent, self.recv.at[3], self.place(self.xl, self.c))

    def near(self):
        left, right, other = self.at(self.xl), self.at(self.xr), self.place(self.x, 1 - self.c)
        send(left, left, self.sent, self.drecv.at[1], other)
        send(right, right, self.sent, self.drecv.at[2], other)

    def across(self, k):
        half, rest = self.buf.shape[1] // 2, k % 2
        piece = self.buf.at[((self.x + NX - 1 + 2 * (k // 2)) % NX) * NC + self.c, pl.ds(pl.multiple_of(rest * half, half), half)]
        send(piece, piece, self.sent, self.drecv.at[4 + k], self.place(self.x, 1 - self.c))

    def last(self):
        far, other = self.at(self.xa), self.place(self.x, 1 - self.c)
        landed(self.first(far), self.recv.at[2])
        landed(self.second(far), self.recv.at[3])
        send(far, far, self.sent, self.drecv.at[3], other)

    def finish(self):
        for k, at in enumerate((self.x, self.xl, self.xr, self.xa)):
            if self.split and 0 < k < 3:
                half = self.buf.shape[1] // 2
                for j in range(2):
                    landed(self.at(at, 1 - self.c).at[pl.ds(j * half, half)], self.drecv.at[2 + 2 * k + j])
            else:
                landed(self.at(at, 1 - self.c), self.drecv.at[k])

    def drain(self):
        landed(self.buf.at[pl.ds(0, 7)], self.sent)


def attend(qs, m, acc, k, v, sbuf, block, starts):
    n = len(starts)
    width = k.shape[0]
    v1 = jnp.concatenate([v, jnp.ones(v.shape, v.dtype)], axis=1)

    def scores(i):
        return lax.dot_general(qs[pl.ds(starts[i], block), :], k, NT, preferred_element_type=F32)

    sbuf[0, :, :width] = scores(0)
    for i in range(n):
        if i + 1 < n:
            sbuf[(i + 1) % 2, :, :width] = scores(i + 1)
        rows = pl.ds(starts[i], block)
        s = sbuf[i % 2, :, :width]
        before = m[rows, :]
        after = jnp.maximum(before, jnp.max(s, axis=1, keepdims=True))
        p = jnp.exp2(s - after[:, :1]).astype(BF16)
        rescale = jnp.exp2(before - after)
        m[rows, :] = after
        pv = jnp.dot(p, v1, preferred_element_type=F32)
        acc[rows, :] = acc[rows, :] * jnp.concatenate([rescale, rescale], axis=1) + pv


def kernel(
    tok, ctxr,
    lat_h, ctx_h, cl_h, cc_h, shw_h, scw_h, gaw_h, gain_h, lam_h, rowt_h, colt_h, wq, wk, wv, wo, out,
    lat, ctx, cond, modm, small, lam_s, rowt, colt, cos, sin,
    zbuf, ybuf, tbuf, modw, inv, lbuf, hid, w, wall, qst, kst, vst, qbuf, kv, qs, m, acc, sbuf, obuf, hb,
    wsem, vec_s, vec_r, gather_s, l_r, l_dr, w_r, w_dr,
    q_s, q_r, k_s, v_s, kv_r, kv_s, ring_r, d_r, o_s, o_r,
):
    sp, tp = lax.axis_index("sp"), lax.axis_index("tp")
    z, y = sp // NY, sp % NY
    x, c = tp // NC, tp % NC

    def place(px, pc, py=None, pz=None):
        return ((z if pz is None else pz) * NY + (y if py is None else py), px * NC + pc)

    pairs = [
        (lat_h, lat), (cl_h, cond.at[pl.ds(0, 1)]), (cc_h, cond.at[pl.ds(1, 1)]),
        (shw_h, modm.at[0]), (scw_h, modm.at[1]), (gaw_h, modm.at[2]),
        (rowt_h, rowt), (colt_h, colt), (ctx_h, ctx), (gain_h, small), (lam_h, lam_s),
        (wk.at[0], w.at[:, pl.ds(256, 128)]), (wk.at[1], w.at[:, pl.ds(384, 128)]),
        (wv, w.at[:, pl.ds(512, 256)]),
        (wq.at[0], w.at[:, pl.ds(0, 128)]), (wq.at[1], w.at[:, pl.ds(128, 128)]),
        (wo, wall.at[tp]),
    ]
    group = [0, 1, 1, 2, 2, 2, 3, 4, 5, 6, 7, 8, 8, 8, 8, 8, 9]
    loads = [pltpu.make_async_copy(src, dst, wsem.at[group[k]]) for k, (src, dst) in enumerate(pairs)]

    barrier = pltpu.get_barrier_semaphore()
    others = [(dx, dy, dc) for dx in range(NX) for dy in range(NY) for dc in range(NC)][1:]
    for dz in range(1, NZ):
        pl.semaphore_signal(barrier, inc=1, device_id=place(x, c, pz=(z + dz) % NZ), device_id_type=MESH)
    for dx, dy, dc in others:
        pl.semaphore_signal(
            barrier, inc=1, device_id=place((x + dx) % NX, (c + dc) % NC, py=(y + dy) % NY), device_id_type=MESH
        )
    for load in loads:
        load.start()
    landed(lat, wsem.at[0])
    landed(cond, wsem.at[1])
    landed(modm, wsem.at[2])

    span = modm.shape[1]
    v = cond[:, pl.ds(pl.multiple_of(sp // 2 * 128, 128), 128)]
    v = v / (1.0 + jnp.exp(-v))
    v = jnp.where(sp % 2 == 0, v, pltpu.roll(v, 128 - span, 1))[:, :span]
    row = lax.broadcasted_iota(jnp.int32, (16, span), 0)
    first, second, none = v[0:1], v[1:2], jnp.zeros((16, span), F32)

    def left(k):
        return jnp.where(row == k, first, jnp.where(row == k + 1, second, none)).astype(BF16)

    part = jnp.dot(left(0), modm[0], preferred_element_type=F32)
    part += jnp.dot(left(2), modm[1], preferred_element_type=F32)
    part += jnp.dot(jnp.where(row == 4, first, none).astype(BF16), modm[2], preferred_element_type=F32)
    zbuf[0] = part[:8]
    lbuf[tp] = lat[...]

    for load in loads[6:11]:
        load.wait()
    in_row = lax.broadcasted_iota(jnp.int32, (GRID_W, 128), 1) % 32 < 16
    for k in range(tok // GRID_W):
        r = sp * (tok // GRID_W) + k
        cos[k * GRID_W : (k + 1) * GRID_W, :] = jnp.where(in_row, rowt[0, pl.ds(r, 1), :], colt[0])
        sin[k * GRID_W : (k + 1) * GRID_W, :] = jnp.where(in_row, rowt[1, pl.ds(r, 1), :], colt[1])
    cos[tok : tok + ctxr, :] = jnp.ones((ctxr, 128), F32)
    sin[tok : tok + ctxr, :] = jnp.zeros((ctxr, 128), F32)
    lines = lax.broadcasted_iota(jnp.int32, (8, 256), 0)
    lane = lax.broadcasted_iota(jnp.int32, (8, 256), 1)
    lam = jnp.where(lane < VALUE_DIM, lam_s[0], lam_s[1])
    extra = jnp.where(lines == 5, small[...], jnp.where(lines == 6, lam, jnp.zeros((8, 256), F32)))

    pl.semaphore_wait(barrier, NZ - 1 + len(others))

    for d in range(1, NZ):
        send(zbuf.at[0], zbuf.at[d], vec_s.at[0], vec_r.at[0], place(x, c, pz=(z + d) % NZ))
    rows = Around(
        lbuf, lambda r: r.at[:, pl.ds(0, 1024)], lambda r: r.at[:, pl.ds(1024, 1024)], (gather_s.at[0], l_r, l_dr), x, c, place
    )
    rows.start(lat)
    landed(zbuf.at[pl.ds(1, NZ - 1)], vec_r.at[0])
    total = zbuf[0]
    for k in range(1, NZ):
        total += zbuf[k]
    ybuf[0] = total
    for d in range(1, NY):
        send(ybuf.at[0], ybuf.at[d], vec_s.at[1], vec_r.at[1], place(x, c, py=(y + d) % NY))
    rows.forward()
    landed(ybuf.at[pl.ds(1, NY - 1)], vec_r.at[1])
    tbuf[tp] = (ybuf[0] + ybuf[1]) + (ybuf[2] + ybuf[3]) + extra
    tps = [(dx, dc) for dx in range(NX) for dc in range(NC)][1:]
    for k, (dx, dc) in enumerate(tps):
        send(tbuf.at[tp], tbuf.at[tp], vec_s.at[2], vec_r.at[2 + k], place((x + dx) % NX, (c + dc) % NC))
    rows.near()
    own_rows = lat.shape[0]

    def inverse_of(values):
        values = values.astype(F32)
        return lax.rsqrt(jnp.mean(values * values, axis=-1, keepdims=True) + norm_eps)

    def one_inverse(k):
        rows_of = pl.ds(pl.multiple_of(k * own_rows, 16), own_rows)
        inv[rows_of, :] = jnp.broadcast_to(inverse_of(lbuf[k]), (own_rows, 128))

    def three(k, _):
        one_inverse((x + NX - 1 + k) % NX * NC + c)
        return 0

    def four(k, _):
        one_inverse(k * NC + 1 - c)
        return 0

    lax.fori_loop(0, 3, three, 0)
    rows.last()
    rows.finish()

    loads[16].wait()
    weights = Around(
        wall, lambda r: r.at[pl.ds(0, 128)], lambda r: r.at[pl.ds(128, 128)], (gather_s.at[1], w_r, w_dr), x, c, place, True
    )
    weights.start(wall.at[tp])

    def modulate(values, inverse, shift, scale):
        return (values.astype(F32) * inverse * (1.0 + scale) + shift).astype(BF16)


    one_inverse((x + 2) % NX * NC + c)
    lax.fori_loop(0, NX, four, 0)
    inv[tok : tok + ctxr, :] = jnp.broadcast_to(inverse_of(ctx[...]), (ctxr, 128))
    for k, (dx, dc) in enumerate(tps):
        landed(tbuf.at[((x - dx + NX) % NX) * NC + (c + dc) % NC], vec_r.at[2 + k])
    for k in range(NX * NC):
        modw[:, k * 256 : (k + 1) * 256] = tbuf[k]

    def one_block(k, _):
        rows_of = pl.ds(pl.multiple_of(k * own_rows, 16), own_rows)
        hid[rows_of, :] = modulate(lbuf[k], inv[rows_of, :][:, :1], modw[0:1, :], modw[2:3, :])
        return 0

    lax.fori_loop(0, NX * NC, one_block, 0)
    hid[tok : tok + ctxr, :] = modulate(ctx[...], inv[tok : tok + ctxr, :][:, :1], modw[1:2, :], modw[3:4, :])
    landed(w, wsem.at[8])

    lane = lax.broadcasted_iota(jnp.int32, (tok + ctxr, 128), 1)
    low_half, low_head = lane % 64 < 32, lane < 64

    def turned(u):
        swapped = jnp.where(low_half, pltpu.roll(u, 96, 1), pltpu.roll(u, 32, 1))
        return u * cos[...] + swapped * sin[...]

    def by_head(both):
        m1, m2 = turned(both[:, :128]), turned(both[:, 128:])
        return (
            jnp.where(low_head, m1, pltpu.roll(m2, 64, 1)),
            jnp.where(low_head, pltpu.roll(m1, 64, 1), m2),
        )

    near, rest = (y + 1) % 2, y % 2
    ynear, yrest = 2 * c + near, 2 * c + rest
    here = yrest == y

    def to_near(stage, sems, part):
        off = (y - ynear + NY) % NY
        send(stage.at[near], kv.at[part, z, off], sems.at[0], kv_r.at[off], place(x, part, py=ynear))

        @pl.when(jnp.logical_and(here, c == part))
        def _():
            kv[part, z, 0] = stage[rest]

        @pl.when(jnp.logical_and(here, c != part))
        def _():
            send(stage.at[rest], kv.at[part, z, 0], sems.at[1], kv_r.at[0], place(x, part))

    def to_far(stage, sems, part):
        @pl.when(jnp.logical_not(here))
        def _():
            send(stage.at[rest], kv.at[part, z, 2], sems.at[1], kv_r.at[2], place(x, part, py=yrest))

    vals = jnp.dot(hid[...], w[:, 512:768], preferred_element_type=F32).astype(BF16)
    vst[0], vst[1] = vals[:, :128], vals[:, 128:]
    to_near(vst, v_s, 1)
    keys = by_head(jnp.dot(hid[...], w[:, 256:512], preferred_element_type=F32))
    kst[0], kst[1] = keys[0].astype(BF16), keys[1].astype(BF16)
    to_near(kst, k_s, 0)
    to_far(vst, v_s, 1)
    to_far(kst, k_s, 0)

    up, down, other = place(x, c, pz=(z + 1) % NZ), place(x, c, pz=(z + NZ - 1) % NZ), place(x, 1 - c)

    def own(o):
        if o == 0:

            @pl.when(c != y // 2)
            def _():
                landed(kv.at[c, z, 0], kv_r.at[0])
        else:
            landed(kv.at[c, z, o], kv_r.at[o])
        mine = kv.at[c, z, o]
        send(mine, mine, kv_s.at[0], ring_r.at[0, 0, o], up)
        send(mine, mine, kv_s.at[0], ring_r.at[1, 0, o], down)
        send(mine, mine, kv_s.at[2], d_r.at[0, o // 2], other)

    own(0)
    heads = by_head(jnp.dot(hid[...], w[:, 0:256], preferred_element_type=F32))
    for j in range(2):
        qst[j] = (heads[j][:tok] * (log2_e * HEAD_DIM**-0.5)).astype(BF16)
    send(qst.at[near], qbuf.at[y % 2], q_s.at[0], q_r.at[y % 2], place(x, y // 2, py=ynear))

    @pl.when(here)
    def _():
        qbuf[y % 2] = qst[rest]

    @pl.when(jnp.logical_not(here))
    def _():
        send(qst.at[rest], qbuf.at[y % 2], q_s.at[1], q_r.at[y % 2], place(x, y // 2, py=yrest))

    m[...] = jnp.full(m.shape, -jnp.inf, F32)
    acc[...] = jnp.zeros(acc.shape, F32)
    for o in (1, 3, 2):
        own(o)
    for i in range(2):

        @pl.when(2 * c + i != y)
        def _():
            landed(qbuf.at[i], q_r.at[i])

    low = lax.broadcasted_iota(jnp.int32, (tok, 128), 1) < 64
    for i in range(2):
        q = qbuf[i]
        nothing = jnp.zeros_like(q)
        qs[i * tok : (i + 1) * tok, :] = jnp.where(low, q, nothing)
        qs[(2 + i) * tok : (3 + i) * tok, :] = jnp.where(low, nothing, q)
    order = [k * tok + b for k in range(4) for b in range(0, tok, 128)]

    def places(u):
        far, p = (u + 1) // 2, (u + 1) % 2
        return far, p, p * ((u + 6) // 7), ((z - far + NZ) % NZ, (z + far) % NZ)

    def pass_on(u, q):
        far, p, _, froms = places(u)
        o = 2 * p + q
        for side in range(2):
            piece = kv.at[c, froms[side], o]
            landed(piece, ring_r.at[side, far - 1, o])

            @pl.when(jnp.logical_or(far < 3, c == side))
            def _():
                send(piece, piece, kv_s.at[1], ring_r.at[side, far, o], up if side == 0 else down)

            send(piece, piece, kv_s.at[2], d_r.at[u, side], other)

    opposite = (z + NZ // 2) % NZ

    def opposite_lands(p):
        for o in (2 * p, 2 * p + 1):
            piece = kv.at[c, opposite, o]
            landed(piece, ring_r.at[c, 3, o])
            send(piece, piece, kv_s.at[2], d_r.at[7, p], other)

    def unit(u, _):
        @pl.when(u < 6)
        def _():
            pass_on(u + 1, 0)

        @pl.when(u == 6)
        def _():
            opposite_lands(0)

        _, p, first, froms = places(u)
        landed(kv.at[1 - c, froms[0], pl.ds(2 * first, 2)], d_r.at[u, 0])
        landed(kv.at[1 - c, froms[1], pl.ds(2 * p, 2)], d_r.at[u, 1])
        k, v = (
            jnp.concatenate(
                [
                    kv[part, froms[0], pl.ds(2 * first, 2), 0:tok, :].reshape(2 * tok, 128),
                    kv[part, froms[1], pl.ds(2 * p, 2), 0:tok, :].reshape(2 * tok, 128),
                ]
            )
            for part in range(2)
        )
        attend(qs, m, acc, k, v, sbuf, 128, order[:6])
        @pl.when(u < 6)
        def _():
            pass_on(u + 1, 1)

        @pl.when(u == 6)
        def _():
            opposite_lands(1)

        @pl.when(u == 3)
        def _():
            weights.forward()

        @pl.when(u >= 3)
        def _():
            weights.across(u - 3)

        attend(qs, m, acc, k, v, sbuf, 128, order[6:])
        return 0

    lax.fori_loop(0, 7, unit, 0)

    def finish(i):
        r1, r2 = pl.ds(i * tok, tok), pl.ds((2 + i) * tok, tok)
        mine = tbuf[2 * x + y // 2]
        picked = jnp.where(y % 2 == 0, mine[:, :128], mine[:, 128:])
        gain, factor = picked[5:6, :], picked[6:7, :]
        mixed = acc[r1, :128] / acc[r1, 128:] - factor * (acc[r2, :128] / acc[r2, 128:])
        normed = mixed * lax.rsqrt(jnp.mean(mixed * mixed, axis=-1, keepdims=True) + norm_eps) * gain
        obuf[i] = normed.astype(BF16).reshape(obuf.shape[1:])
        head = NY * x + y
        for t in range(NX * NC):
            home = jnp.logical_and(2 * c + i == y, tp == t)

            @pl.when(jnp.logical_not(home))
            def _():
                send(obuf.at[i, t], hb.at[head], o_s.at[0], o_r.at[head // 2], (z * NY + 2 * c + i, t))

            @pl.when(home)
            def _():
                hb[head] = obuf[i, t]

    for p in range(2):
        landed(kv.at[1 - c, opposite, pl.ds(2 * p, 2)], d_r.at[7, p])
    k, v = (
        jnp.concatenate(
            [
                kv[part, opposite, :, 0:tok, :].reshape(NY * tok, 128),
                kv[part, :, :, tok : tok + ctxr, :].reshape(NZ * NY * ctxr, 128),
            ]
        )
        for part in range(2)
    )
    for i in range(2):
        attend(qs, m, acc, k, v, sbuf, 128, [k2 * tok + b for k2 in (i, 2 + i) for b in range(0, tok, 128)])
        finish(i)
        if i == 0:
            weights.last()
    weights.finish()
    mixed_sum = jnp.zeros((own_rows, wall.shape[2]), F32)
    for dx in (0, 1, 3, 2):
        hx = (x + dx) % NX
        for half in range(2):
            g = 2 * hx + half
            if dx == 0:

                @pl.when(jnp.logical_and(c == half, y // 2 == half))
                def _():
                    landed(hb.at[2 * g + 1 - y % 2], o_r.at[g])

                @pl.when(jnp.logical_not(jnp.logical_and(c == half, y // 2 == half)))
                def _():
                    landed(hb.at[pl.ds(2 * g, 2)], o_r.at[g])
            else:
                landed(hb.at[pl.ds(2 * g, 2)], o_r.at[g])
            pair = jnp.concatenate([hb[2 * g], hb[2 * g + 1]], axis=1)
            mixed_sum += jnp.dot(pair, wall[g], preferred_element_type=F32).astype(BF16).astype(F32)
    out[...] = (lat[...].astype(F32) + modw[4:5, :] * mixed_sum).astype(BF16)

    landed(zbuf.at[pl.ds(0, NZ - 1)], vec_s.at[0])
    landed(ybuf.at[pl.ds(0, NY - 1)], vec_s.at[1])
    landed(tbuf.at[pl.ds(0, len(tps))], vec_s.at[2])
    rows.drain()
    weights.drain()
    landed(qst.at[0], q_s.at[0])
    landed(kst.at[0], k_s.at[0])
    landed(vst.at[0], v_s.at[0])

    @pl.when(jnp.logical_not(here))
    def _():
        landed(qst.at[1], q_s.at[1])

    @pl.when(jnp.logical_or(jnp.logical_not(here), c != 0))
    def _():
        landed(kst.at[1], k_s.at[1])

    @pl.when(jnp.logical_or(jnp.logical_not(here), c != 1))
    def _():
        landed(vst.at[1], v_s.at[1])

    landed(kv.at[c, pl.ds(0, 2)], kv_s.at[0])
    landed(kv.at[c, pl.ds(0, 5)], kv_s.at[1])
    landed(kv.at[c], kv_s.at[2])

    @pl.when(c == y // 2)
    def _():
        landed(hb.at[pl.ds(0, NX * NY - 1)], o_s.at[0])

    @pl.when(c != y // 2)
    def _():
        landed(hb, o_s.at[0])


def tables(grid_rows):
    quarter = HEAD_DIM // 4
    inverse = np.float32(rope_theta) ** (-np.arange(quarter, dtype=np.float32) / np.float32(quarter))
    sign = np.array([-1.0, 1.0, -1.0, 1.0]).repeat(2 * quarter)

    def table(count):
        angles = (np.arange(count, dtype=np.float32)[:, None] * inverse).astype(np.float64)
        cos, sin = np.tile(np.cos(angles), (1, 8)), np.tile(np.sin(angles), (1, 8)) * sign
        return jnp.asarray(np.stack([cos, sin]).astype(np.float32))

    return table(grid_rows), table(GRID_W)


def local(
    latent, context, cond_latent, cond_context, shift_weight, scale_weight, gate_weight,
    query_weight, key_weight, value_weight, out_weight, lambda_heads, out_gain,
):
    own_rows, width = latent.shape
    ctxr = context.shape[0]
    tok = own_rows * NX * NC
    rowt, colt = tables(tok * lax.axis_size("sp") // GRID_W)
    hbm = pl.BlockSpec(memory_space=pl.ANY)
    dma = pltpu.SemaphoreType.DMA
    return pl.pallas_call(
        functools.partial(kernel, tok, ctxr),
        out_shape=jax.ShapeDtypeStruct((own_rows, width), BF16),
        in_specs=[hbm] * 15,
        out_specs=pl.BlockSpec(memory_space=pltpu.VMEM),
        scratch_shapes=[
            pltpu.VMEM((own_rows, width), BF16),
            pltpu.VMEM((ctxr, width), BF16),
            pltpu.VMEM((2, width), F32),
            pltpu.VMEM((3, *shift_weight.shape), BF16),
            pltpu.VMEM((1, 256), F32),
            pltpu.SMEM(lambda_heads.shape, F32),
            pltpu.VMEM(rowt.shape, F32),
            pltpu.VMEM(colt.shape, F32),
            pltpu.VMEM((tok + ctxr, 128), F32),
            pltpu.VMEM((tok + ctxr, 128), F32),
            pltpu.VMEM((NZ, 8, 256), F32),
            pltpu.VMEM((NY, 8, 256), F32),
            pltpu.VMEM((NX * NC, 8, 256), F32),
            pltpu.VMEM((8, width), F32),
            pltpu.VMEM((tok + ctxr, 128), F32),
            pltpu.VMEM((NX * NC, own_rows, width), BF16),
            pltpu.VMEM((tok + ctxr, width), BF16),
            pltpu.VMEM((width, 768), BF16),
            pltpu.VMEM((NX * NC, 256, width), BF16),
            pltpu.VMEM((2, tok, 128), BF16),
            pltpu.VMEM((2, tok + ctxr, 128), BF16),
            pltpu.VMEM((2, tok + ctxr, 128), BF16),
            pltpu.VMEM((2, tok, 128), BF16),
            pltpu.VMEM((2, NZ, NY, tok + ctxr, 128), BF16),
            pltpu.VMEM((4 * tok, 128), BF16),
            pltpu.VMEM((4 * tok, 128), F32),
            pltpu.VMEM((4 * tok, 256), F32),
            pltpu.VMEM((2, 128, NY * (tok + NZ * ctxr)), F32),
            pltpu.VMEM((2, NX * NC, own_rows, 128), BF16),
            pltpu.VMEM((NX * NY, own_rows, 128), BF16),
            dma((10,)), dma((3,)), dma((9,)), dma((2,)), dma((4,)), dma((4,)), dma((4,)), dma((8,)),
            dma((2,)), dma((2,)), dma((2,)), dma((2,)), dma((NY,)),
            dma((3,)), dma((2, 4, NY)), dma((NZ, 2)), dma((1,)), dma((NX * NC,)),
        ],
        compiler_params=pltpu.CompilerParams(
            collective_id=0, has_side_effects=True, vmem_limit_bytes=60 * 2**20
        ),
    )(
        latent, context, cond_latent[None], cond_context[None], shift_weight, scale_weight, gate_weight,
        out_gain[None], lambda_heads, rowt, colt, query_weight, key_weight, value_weight, out_weight,
    )


def solution(mesh):
    placed = (
        P(("sp", "tp"), None), P("sp", None), P(), P(),
        P("sp", "tp"), P("sp", "tp"), P("sp", "tp"),
        P(None, None, "tp"), P(None, None, "tp"), P(None, "tp"), P("tp", None), P("tp"), P("tp"),
    )
    return jax.shard_map(
        local, mesh=mesh, in_specs=placed, out_specs=P(("sp", "tp"), None), check_vma=False
    )
```
